512 devices in a mesh: sp: 32 (over z, x), tp: 16 (over y, core).
Axes of the slice: x: 4, y: 8, z: 8, core: 2. Of those that a mesh axis runs over, the one named last changes fastest.
Arguments:
- resid: bfloat16 [16384, 2048], P(('sp', 'tp')), may hold values from -6 to 6
- recurrent_input: bfloat16 [16384, 2048], P('sp', 'tp'), may hold values from -12.2 to 12.2
- recurrent_out_gate: bfloat16 [16384, 2048], P('sp', 'tp'), may hold values from -6 to 6
- filter_weight: float32 [4, 2048], P(None, 'tp'), may hold values from -3 to 3
- recurrence_gate_matrix: bfloat16 [32, 64, 64], P('tp'), may hold values from -0.75 to 0.75
- input_gate_matrix: bfloat16 [32, 64, 64], P('tp'), may hold values from -0.75 to 0.75
- channel_decay_raw: float32 [2048], P('tp'), may hold values from 4.8 to 13.5
- token_decay_boost: float32 [16384, 2048], P('sp', 'tp'), may hold values from -0.7 to 0
- output_projection_weight: bfloat16 [2048, 2048], P('tp'), may hold values from -0.375 to 0.375
- expert_norm_gain: float32 [2048], replicated, may hold values from 0.1 to 1.9
- routes: int32 [16384, 2], P('sp'), may hold values from 0 to 31, all different within a row; in each aligned block of 32 rows (0 to 31, 32 to 63, ...) at most 3 rows name the same one
- expert_pair_weight: float32 [16384, 2], P(('sp', 'tp')), may hold values from 0.2 to 0.8
- gate_weight: bfloat16 [32, 2048, 2048], P('sp', None, 'tp'), may hold values from -0.125 to 0.125
- up_weight: bfloat16 [32, 2048, 2048], P('sp', None, 'tp'), may hold values from -0.125 to 0.125
- down_weight: bfloat16 [32, 2048, 2048], P('sp', None, 'tp'), may hold values from -0.25 to 0.25
Outputs:
- layer_out: bfloat16 [16384, 2048], P(('sp', 'tp'))
The draws below stay inside these ranges and needn't reach their ends.
Inputs may be any that keep to these rules, and one draw needn't show every extreme that they name: `routes`: in each aligned block of 32 rows no expert is named by more than 3 rows, and the two experts of a row differ.
All inputs are finite; a program needn't handle non-finite values.
Results may differ from the reference program's by a relative error of at most 0.013.
Values may be sent and summed in bfloat16 or wider, within the bound.
No kernel may reach another device: no remote copies, remote signals or barrier semaphores. Data moves between devices by JAX's collectives and lax.ppermute only.
A program may use at most 64 MiB of HBM per device.

```python
import math
import jax
import jax.numpy as jnp
import numpy as np
from jax import lax

D = 2048
LRU = 2048
BW = 64
HID = 2048
CONV = 4
TOK_SP = 512
BLOCKS = 32
TOKENS = 16384
ROWS_DEV = 32
EXPERTS = 32
CAP = 3
ROWS_ALL = 1536


def draw_recurrent_input(key, part):
    base_key, scale_key = jax.random.split(jax.random.fold_in(key, 11))
    base = jnp.clip(jax.random.normal(base_key, (TOKENS, LRU), jnp.float32), -6.0, 6.0)
    block_scale = jnp.exp(jax.random.uniform(scale_key, (TOKENS // TOK_SP, 1), jnp.float32, -0.7, 0.7))
    return (base * jnp.repeat(block_scale, TOK_SP, axis=0)).astype(jnp.bfloat16)


def draw_channel_decay_raw(key, part):
    pick_key, fast_key, slow_key = jax.random.split(jax.random.fold_in(key, 12), 3)
    share = 0.5
    fast = jax.random.uniform(pick_key, (LRU,), jnp.float32) < share
    quick = jax.random.uniform(fast_key, (LRU,), jnp.float32, 4.8, 6.0)
    steady = jax.random.uniform(slow_key, (LRU,), jnp.float32, 11.0, 13.5)
    return jnp.where(fast, quick, steady)


def draw_token_decay_boost(key, part):
    place_key, size_key = jax.random.split(jax.random.fold_in(key, 13))
    places = jax.random.randint(place_key, (3, LRU), 0, TOKENS)
    drops = jax.random.uniform(size_key, (3, LRU), jnp.float32, -0.7, -0.22)
    position = jnp.arange(TOKENS)[:, None]
    result = jnp.zeros((TOKENS, LRU), jnp.float32)
    for number in range(3):
        result = jnp.minimum(result, jnp.where(position == places[number][None, :], drops[number][None, :], 0.0))
    return result


def level_of(key, shape, cuts, least, high):
    loudness, own = 1.0, jax.random.fold_in(key, 6)
    for dim, blocks in cuts:
        steps = jnp.exp(jax.random.uniform(jax.random.fold_in(own, dim), (blocks,), jnp.float32, least / len(cuts), high / len(cuts)))
        loudness = loudness * jnp.repeat(steps, shape[dim] // blocks).reshape([-1 if axis == dim else 1 for axis in range(len(shape))])
    return loudness


def routed_block(own_key, own, number, rows, amount, top, limit, slope):
    ranking = jax.random.permutation(own_key, amount)
    packed, ordinary = shares(amount, rows * top, limit, slope, True), shares(amount, rows * top, limit, slope, False)
    places = jnp.arange(amount)

    def named(tallies, rotation):
        used = int((tallies > 0).sum())
        fixed = max(1, used // 4)
        shifted = fixed + (places - fixed + rotation * (used - fixed)) % max(1, amount - fixed)
        return jnp.zeros((amount,), jnp.int32).at[ranking[jnp.where(places < fixed, places, shifted)]].set(jnp.asarray(tallies, jnp.int32))

    tallies = jnp.where(number % 4 == 0, named(packed, number // 4), named(ordinary, number - number // 4 - 1))
    mixed = jax.random.permutation(jax.random.fold_in(own, 3), amount)
    donor, sink = mixed[0:amount // 2 * 2:2], mixed[1:amount // 2 * 2:2]
    margin = jnp.minimum(tallies[donor] - 1, limit - tallies[sink]) // 2
    margin = jnp.where((donor == ranking[0]) | (sink == ranking[0]) | (tallies[sink] == 0), 0, jnp.maximum(margin, 0))
    shifted = jax.random.randint(jax.random.fold_in(own, 4), (amount // 2,), 0, 1 << 20) % (margin + 1)
    tallies = tallies.at[donor].add(-shifted).at[sink].add(shifted)
    labels = jnp.searchsorted(jnp.cumsum(tallies), jnp.arange(rows * top), side="right").astype(jnp.int32)
    listing = labels.reshape(top, rows).T
    listing = listing[jax.random.permutation(jax.random.fold_in(own, 1), rows)]
    rotation = jax.random.randint(jax.random.fold_in(own, 2), (rows, 1), 0, top)
    return jnp.take_along_axis(listing, (jnp.arange(top)[None, :] + rotation) % top, axis=1)


def shares(amount, total, bound, slope, full):
    portions = [(1 << 20) // math.isqrt(standing ** slope) + 1 for standing in range(1, amount + 1)]
    largest = bound if full else min(bound, max(-(-total // amount), total * portions[0] // sum(portions)))
    least = 1 if total - largest >= amount - 1 else 0
    counts, rest = [largest] + [least] * (amount - 1), total - largest - least * (amount - 1)
    while rest > 0:
        candidates = [i for i in range(1, amount) if counts[i] < largest] or [i for i in range(1, amount) if counts[i] < bound]
        mass, remaining = sum([portions[i] for i in candidates]), rest
        for i in candidates:
            extra = min(bound - counts[i], max(1, remaining * portions[i] // mass), rest)
            counts[i] = counts[i] + extra
            rest = rest - extra
    return np.array(counts)


def normal_values(rng, extent, scale, reach, shards=(), kind=jnp.bfloat16):
    drawn = scale * jax.random.normal(rng, extent, jnp.float32)
    if shards:
        drawn = drawn * level_of(rng, extent, shards, -0.22, 0.18)
    return jnp.clip(drawn, -reach, reach).astype(kind)


def setup_inputs(seed: int = 0) -> dict:
    splits = jax.random.split(jax.random.key(seed), 16)
    resid = normal_values(splits[0], (TOKENS, D), 1.0, 6.0, ((0, 512),))
    recurrent_input = draw_recurrent_input(jax.random.fold_in(splits[15], 71), 0)
    recurrent_out_gate = normal_values(splits[2], (TOKENS, LRU), 1.0, 6.0, ((0, 32), (1, 16)))
    filter_weight = normal_values(splits[3], (CONV, LRU), 0.5, 3.0, ((1, 16),), jnp.float32)
    recurrence_gate_matrix = normal_values(splits[4], (BLOCKS, BW, BW), BW ** -0.5, 0.75, ((0, 16),))
    input_gate_matrix = normal_values(splits[5], (BLOCKS, BW, BW), BW ** -0.5, 0.75, ((0, 16),))
    channel_decay_raw = draw_channel_decay_raw(jax.random.fold_in(splits[15], 71), 0)
    token_decay_boost = draw_token_decay_boost(jax.random.fold_in(splits[15], 71), 0)
    output_projection_weight = normal_values(splits[8], (LRU, D), (LRU // 9) ** -0.5, 0.375, ((0, 16),))
    expert_norm_gain = jnp.clip(1.0 + 0.18 * jax.random.normal(splits[9], (D,), jnp.float32), 0.1, 1.9)
    routes_keys = jax.random.split(jax.random.fold_in(splits[10], 1), TOKENS // ROWS_DEV)
    routes_turns = jax.random.permutation(jax.random.fold_in(splits[10], 3), TOKENS // ROWS_DEV)
    routes = jax.vmap(lambda own, number: routed_block(jax.random.fold_in(splits[10], 2), own, number, ROWS_DEV, EXPERTS, 2, CAP, 1))(routes_keys, routes_turns).reshape((TOKENS, 2))
    expert_pair_weight = jnp.clip(0.2 + 0.6 * jax.random.uniform(splits[11], (TOKENS, 2), jnp.float32) ** level_of(splits[11], (TOKENS, 2), ((0, 512),), -0.2, 0.2), 0.2, 0.8)
    gate_weight = normal_values(splits[12], (EXPERTS, D, HID), D ** -0.5, 0.125, ((0, 32), (2, 16)))
    up_weight = normal_values(splits[13], (EXPERTS, D, HID), D ** -0.5, 0.125, ((0, 32), (2, 16)))
    down_weight = normal_values(splits[14], (EXPERTS, HID, D), (HID // 4) ** -0.5, 0.25, ((0, 32), (2, 16)))
    return dict(resid=resid, recurrent_input=recurrent_input, recurrent_out_gate=recurrent_out_gate, filter_weight=filter_weight, recurrence_gate_matrix=recurrence_gate_matrix, input_gate_matrix=input_gate_matrix, channel_decay_raw=channel_decay_raw, token_decay_boost=token_decay_boost, output_projection_weight=output_projection_weight, expert_norm_gain=expert_norm_gain, routes=routes, expert_pair_weight=expert_pair_weight, gate_weight=gate_weight, up_weight=up_weight, down_weight=down_weight)


def chain_step(earlier, later):
    return (earlier[0] * later[0], later[0] * earlier[1] + later[1])

def reference(resid, recurrent_input, recurrent_out_gate, filter_weight, recurrence_gate_matrix, input_gate_matrix, channel_decay_raw, token_decay_boost, output_projection_weight, expert_norm_gain, routes, expert_pair_weight, gate_weight, up_weight, down_weight):
    total = recurrent_input.shape[0]
    taps = filter_weight.shape[0]
    padded = jnp.pad(recurrent_input.astype(jnp.float32), ((taps - 1, 0), (0, 0)))
    mixed_in = padded[0:total] * filter_weight[0]
    for offset in range(1, taps):
        mixed_in = mixed_in + padded[offset:offset + total] * filter_weight[offset]
    smoothed = mixed_in.astype(jnp.bfloat16)
    grouped = smoothed.astype(jnp.float32).reshape(total, BLOCKS, BW)
    recurrence_gate = jax.nn.sigmoid(jnp.einsum('tni,nij->tnj', grouped, recurrence_gate_matrix.astype(jnp.float32)).reshape(total, LRU))
    input_gate = jax.nn.sigmoid(jnp.einsum('tni,nij->tnj', grouped, input_gate_matrix.astype(jnp.float32)).reshape(total, LRU))
    decay_logarithm = -8.0 * recurrence_gate * jax.nn.softplus(-channel_decay_raw) + token_decay_boost
    decay = jnp.exp(decay_logarithm)
    drive = jnp.sqrt(-jnp.expm1(2.0 * decay_logarithm)) * (input_gate * smoothed.astype(jnp.float32))
    running, state = lax.associative_scan(chain_step, (decay, drive), axis=0)
    branch = (jax.nn.gelu(recurrent_out_gate.astype(jnp.float32)) * state).astype(jnp.bfloat16)
    projected = jnp.dot(branch, output_projection_weight, preferred_element_type=jnp.float32)
    stream = (resid.astype(jnp.float32) + projected).astype(jnp.bfloat16)
    stream_wide = stream.astype(jnp.float32)
    normed = (stream_wide * lax.rsqrt(lax.optimization_barrier(jnp.mean(stream_wide * stream_wide, axis=1, keepdims=True)) + 1e-06) * expert_norm_gain).astype(jnp.bfloat16)
    flat_routes = routes.reshape(-1)
    flat_weight = expert_pair_weight.reshape(-1)
    slot_index = jnp.arange(ROWS_ALL, dtype=jnp.int32)

    def one_expert(accum, items):
        gate_part, up_part, down_part, number = items
        hits = flat_routes == number
        count = jnp.sum(hits.astype(jnp.int32))
        chosen = jnp.nonzero(hits, size=ROWS_ALL, fill_value=0)[0].astype(jnp.int32)
        valid = slot_index < count
        token = chosen // 2
        rows = normed[token]
        gate = jnp.dot(rows, gate_part, preferred_element_type=jnp.float32)
        upward = jnp.dot(rows, up_part, preferred_element_type=jnp.float32)
        active = (jax.nn.silu(gate) * upward).astype(jnp.bfloat16)
        result = jnp.dot(active, down_part, preferred_element_type=jnp.float32).astype(jnp.bfloat16).astype(jnp.float32)
        factor = jnp.where(valid, flat_weight[chosen], 0.0)
        return (accum.at[token].add(result * factor[:, None]), None)
    start = jnp.zeros((total, D), jnp.float32)
    accum, _ = lax.scan(one_expert, start, (gate_weight, up_weight, down_weight, jnp.arange(EXPERTS, dtype=jnp.int32)))
    return (stream_wide + accum).astype(jnp.bfloat16)
```

```python
import jax
import jax.numpy as jnp
from jax import lax
from jax.experimental import pallas as pl
from jax.experimental.pallas import tpu as pltpu
from jax.sharding import PartitionSpec as P


RECURRENT_SCALE = 8.0
EPSILON = 1e-06
SEGMENTS = 8
CORES = 2
CAP = 3
GELU_SCALE = 0.7978845608028654

VMEM = pl.BlockSpec(memory_space=pltpu.VMEM)
SMEM = pl.BlockSpec(memory_space=pltpu.SMEM)


def shifted(block, axis, distance):
    devices = range(lax.axis_size(axis))
    route = [(i - distance, i) for i in devices if i - distance in devices]
    return lax.ppermute(block, axis, route)


def from_everyone(x, axis):
    size = lax.axis_size(axis)
    return lax.all_to_all(jnp.broadcast_to(x[None], (size, *x.shape)), axis, 0, 0, tiled=True)


def core_groups(size):
    return [[core + CORES * y for y in range(size // CORES)] for core in range(CORES)]


def swap_cores(x):
    size = lax.axis_size("tp")
    return lax.ppermute(x, "tp", [(i, i ^ 1) for i in range(size)])


def minus_expm1(x):
    series = 1.0 + x * (1.0 / 7.0)
    for k in (6, 5, 4, 3, 2):
        series = 1.0 + x * (1.0 / k) * series
    return jnp.where(x > -0.35, -x * series, 1.0 - jnp.exp(x))


def recurrence_kernel(
    x_ref, rim_ref, filter_ref, gates_ref, rate_ref, boost_ref,
    state_ref, running_ref, total_ref, ext, decay, drive,
):
    tokens, channels = x_ref.shape
    taps = filter_ref.shape[0]
    lead = 8
    ext[lead - taps + 1 : lead, :] = rim_ref[...].astype(jnp.float32)
    ext[lead : lead + tokens, :] = x_ref[...].astype(jnp.float32)
    first = lead - taps + 1
    mixed = ext[first : first + tokens, :] * filter_ref[0:1, :]
    for k in range(1, taps):
        mixed = mixed + ext[first + k : first + k + tokens, :] * filter_ref[k : k + 1, :]
    smoothed = mixed.astype(jnp.bfloat16)
    logits = jnp.dot(smoothed, gates_ref[...], preferred_element_type=jnp.float32)
    both = jax.nn.sigmoid(logits)
    log_decay = both[:, :channels] * rate_ref[...] + boost_ref[...]
    decay[...] = jnp.exp(log_decay)
    drive[...] = jnp.sqrt(minus_expm1(2.0 * log_decay)) * (
        both[:, channels:] * smoothed.astype(jnp.float32)
    )
    length = tokens // SEGMENTS

    def step(i, held):
        state, running = held
        rows = pl.ds(i, SEGMENTS, stride=length)
        a, b = decay[rows, :], drive[rows, :]
        state, running = a * state + b, running * a
        state_ref[rows, :] = state
        running_ref[rows, :] = running
        return state, running

    start = (jnp.zeros((SEGMENTS, channels), jnp.float32), jnp.ones((SEGMENTS, channels), jnp.float32))
    state, running = lax.fori_loop(0, length, step, start, unroll=8)
    whole_a, whole_b = running[0:1], state[0:1]
    for k in range(1, SEGMENTS):
        whole_b = running[k : k + 1] * whole_b + state[k : k + 1]
        whole_a = whole_a * running[k : k + 1]
    total_ref[0:1, :] = whole_a
    total_ref[1:2, :] = whole_b


def branch_kernel(place_ref, pieces_ref, state_ref, running_ref, gate_ref, keep_ref, send_ref):
    place, core = place_ref[0], place_ref[1]
    devices, _, channels = pieces_ref.shape
    carry = jnp.zeros((1, channels), jnp.float32)
    for k in range(devices):
        piece = pieces_ref[k]
        carry = jnp.where(k < place, piece[0:1] * carry + piece[1:2], carry)
    length = state_ref.shape[0] // SEGMENTS
    half = length // CORES
    for k in range(SEGMENTS):
        for out, side in ((keep_ref, core), (send_ref, 1 - core)):
            rows = pl.ds(pl.multiple_of(k * length + side * half, half), half)
            state = state_ref[rows, :] + running_ref[rows, :] * carry
            g = gate_ref[rows, :].astype(jnp.float32)
            gelu = 0.5 * g * (1.0 + jnp.tanh(GELU_SCALE * (g + 0.044715 * (g * g * g))))
            out[k * half : (k + 1) * half, :] = (gelu * state).astype(jnp.bfloat16)
        last = (k + 1) * length - 1
        carry = running_ref[last : last + 1, :] * carry + state_ref[last : last + 1, :]


def slots_kernel(routes_ref, slots_ref):
    rows = routes_ref.shape[0]
    experts = 32
    number = lax.broadcasted_iota(jnp.int32, (rows, experts), 1)
    hot = [(routes_ref[:, k : k + 1] == number).astype(jnp.float32) for k in range(2)]
    earlier = (
        lax.broadcasted_iota(jnp.int32, (rows, rows), 1)
        < lax.broadcasted_iota(jnp.int32, (rows, rows), 0)
    ).astype(jnp.float32)
    before = jnp.dot(earlier, hot[0] + hot[1], preferred_element_type=jnp.float32)
    for k in range(2):
        rank = jnp.sum(before * hot[k], axis=1, keepdims=True).astype(jnp.int32)
        slots_ref[:, k : k + 1] = routes_ref[:, k : k + 1] * CAP + rank


def dispatch_kernel(parts_ref, resid_ref, gain_ref, slots_ref, stream_ref, out_ref):
    rows, width = resid_ref.shape
    projected = parts_ref[0].astype(jnp.float32)
    for k in range(1, parts_ref.shape[0]):
        projected = projected + parts_ref[k].astype(jnp.float32)
    stream = (resid_ref[...].astype(jnp.float32) + projected).astype(jnp.bfloat16)
    stream_ref[...] = stream
    wide = stream.astype(jnp.float32)
    mean = jnp.sum(wide * wide, axis=1, keepdims=True) * (1.0 / width)
    normed = (wide * lax.rsqrt(mean + EPSILON) * gain_ref[...]).astype(jnp.bfloat16)
    slot = lax.broadcasted_iota(jnp.int32, (rows, out_ref.shape[0]), 1)
    pick = (slots_ref[:, 0:1] == slot) | (slots_ref[:, 1:2] == slot)
    pick = pick.astype(jnp.float32).T.astype(jnp.bfloat16)
    out_ref[...] = jnp.dot(pick, normed, preferred_element_type=jnp.float32).astype(jnp.bfloat16)


def combine_kernel(stream_ref, returned_ref, slots_ref, weight_ref, out_ref):
    rows = stream_ref.shape[0]
    slot = lax.broadcasted_iota(jnp.int32, (rows, returned_ref.shape[0]), 1)
    total = jnp.zeros(stream_ref.shape, jnp.float32)
    for k in range(2):
        pick = (slots_ref[:, k : k + 1] == slot).astype(jnp.float32).astype(jnp.bfloat16)
        chosen = jnp.dot(pick, returned_ref[...], preferred_element_type=jnp.float32)
        total = total + weight_ref[:, k : k + 1] * chosen
    out_ref[...] = (stream_ref[...].astype(jnp.float32) + total).astype(jnp.bfloat16)


def block_diagonal(blocks):
    count, width, _ = blocks.shape
    rows = [
        jnp.pad(blocks[k], ((0, 0), (k * width, (count - 1 - k) * width))) for k in range(count)
    ]
    return jnp.concatenate(rows, axis=0)


def layer(
    resid,
    recurrent_input,
    recurrent_out_gate,
    filter_weight,
    recurrence_gate_matrix,
    input_gate_matrix,
    channel_decay_raw,
    token_decay_boost,
    output_projection_weight,
    expert_norm_gain,
    routes,
    expert_pair_weight,
    gate_weight,
    up_weight,
    down_weight,
):
    tokens, channels = recurrent_input.shape
    taps = filter_weight.shape[0]
    tp, experts = lax.axis_size("tp"), lax.axis_size("sp")
    here, place = lax.axis_index("tp"), lax.axis_index("sp")
    core = here % CORES
    chips = tp // CORES
    groups = core_groups(tp)
    rows_dev, width = resid.shape
    f32, bf16 = jnp.float32, jnp.bfloat16

    rim = shifted(recurrent_input[tokens - taps + 1 :], "sp", 1)
    gates = jnp.concatenate(
        [block_diagonal(recurrence_gate_matrix), block_diagonal(input_gate_matrix)], axis=1
    )
    rate = (-RECURRENT_SCALE * jax.nn.softplus(-channel_decay_raw))[None, :]

    down_all = lax.all_gather(down_weight[0], "tp")
    projection_other = swap_cores(output_projection_weight)
    gate_other = swap_cores(gate_weight[0])
    up_other = swap_cores(up_weight[0])

    own_routes = lax.dynamic_slice_in_dim(routes, here * rows_dev, rows_dev, 0)
    slots = pl.pallas_call(
        slots_kernel,
        out_shape=jax.ShapeDtypeStruct((rows_dev, 2), jnp.int32),
        in_specs=[VMEM],
        out_specs=VMEM,
        name="slots",
    )(own_routes)

    state, running, total = pl.pallas_call(
        recurrence_kernel,
        out_shape=(
            jax.ShapeDtypeStruct((tokens, channels), f32),
            jax.ShapeDtypeStruct((tokens, channels), f32),
            jax.ShapeDtypeStruct((2, channels), f32),
        ),
        in_specs=[VMEM] * 6,
        out_specs=(VMEM,) * 3,
        scratch_shapes=[
            pltpu.VMEM((tokens + 8, channels), f32),
            pltpu.VMEM((tokens, channels), f32),
            pltpu.VMEM((tokens, channels), f32),
        ],
        cost_estimate=pl.CostEstimate(flops=10**9, bytes_accessed=2**20, transcendentals=0),
        name="recurrence",
    )(recurrent_input, rim, filter_weight, gates, rate, token_decay_boost)

    pieces = from_everyone(total, "sp")
    keep, send = pl.pallas_call(
        branch_kernel,
        out_shape=(jax.ShapeDtypeStruct((tokens // CORES, channels), bf16),) * 2,
        in_specs=[SMEM] + [VMEM] * 4,
        out_specs=(VMEM,) * 2,
        name="branch",
    )(jnp.stack([place, core]).astype(jnp.int32), pieces, state, running, recurrent_out_gate)
    got = swap_cores(send)

    both = jnp.concatenate([keep, got], axis=1)
    projection = jnp.concatenate([output_projection_weight, projection_other], axis=0)
    partial = jnp.dot(both, projection, preferred_element_type=f32).astype(bf16)
    parts = lax.all_to_all(
        partial.reshape(chips, rows_dev, width), "tp", 0, 0, axis_index_groups=groups, tiled=True
    )
    slot_count = experts * CAP
    parts, down_all = lax.optimization_barrier((parts, down_all))
    stream, outgoing = pl.pallas_call(
        dispatch_kernel,
        out_shape=(
            jax.ShapeDtypeStruct((rows_dev, width), bf16),
            jax.ShapeDtypeStruct((slot_count, width), bf16),
        ),
        in_specs=[VMEM] * 4,
        out_specs=(VMEM,) * 2,
        name="dispatch",
    )(parts, resid, expert_norm_gain[None, :], slots)
    arrived = lax.all_to_all(
        outgoing.reshape(experts, CAP, width), "sp", split_axis=0, concat_axis=0, tiled=True
    ).reshape(slot_count, width)

    rows = lax.all_gather(arrived, "tp", axis=0, axis_index_groups=groups, tiled=True)
    gate_both = jnp.concatenate([gate_weight[0], gate_other], axis=1)
    up_both = jnp.concatenate([up_weight[0], up_other], axis=1)
    gate = jnp.dot(rows, gate_both, preferred_element_type=f32)
    upward = jnp.dot(rows, up_both, preferred_element_type=f32)
    active = (jax.nn.silu(gate) * upward).astype(bf16)

    hidden = gate_weight.shape[2]
    down_own = lax.dynamic_slice_in_dim(down_all, here * hidden, hidden, 1)
    down_other = lax.dynamic_slice_in_dim(down_all, (here + 1 - 2 * core) * hidden, hidden, 1)
    down = jnp.concatenate([down_own, down_other], axis=1)
    down = jnp.moveaxis(down, 0, 1).reshape(CORES * hidden, width)
    summed = jnp.dot(active, down, preferred_element_type=f32).astype(bf16)
    result = lax.psum_scatter(
        summed, "tp", scatter_dimension=0, axis_index_groups=groups, tiled=True
    )

    returned = lax.all_to_all(
        result.reshape(experts, CAP, width), "sp", split_axis=0, concat_axis=0, tiled=True
    ).reshape(slot_count, width)
    return pl.pallas_call(
        combine_kernel,
        out_shape=jax.ShapeDtypeStruct((rows_dev, width), bf16),
        in_specs=[VMEM] * 4,
        out_specs=VMEM,
        name="combine",
    )(stream, returned, slots, expert_pair_weight)


def solution(mesh):
    placed = (
        P(("sp", "tp"), None),
        P("sp", "tp"),
        P("sp", "tp"),
        P(None, "tp"),
        P("tp", None, None),
        P("tp", None, None),
        P("tp"),
        P("sp", "tp"),
        P("tp", None),
        P(),
        P("sp", None),
        P(("sp", "tp"), None),
        P("sp", None, "tp"),
        P("sp", None, "tp"),
        P("sp", None, "tp"),
    )
    return jax.shard_map(
        layer, mesh=mesh, in_specs=placed, out_specs=P(("sp", "tp"), None), check_vma=False
    )
```

```python
import jax
import jax.numpy as jnp
from jax import lax
from jax.experimental import pallas as pl
from jax.experimental.pallas import tpu as pltpu
from jax.sharding import PartitionSpec as P


RECURRENT_SCALE = 8.0
EPSILON = 1e-06
SEGMENTS = 8
CORES = 2
CAP = 3
PIECES = 8
GELU_SCALE = 0.7978845608028654

VMEM = pl.BlockSpec(memory_space=pltpu.VMEM)
SMEM = pl.BlockSpec(memory_space=pltpu.SMEM)


def shifted(block, axis, distance):
    devices = range(lax.axis_size(axis))
    route = [(i - distance, i) for i in devices if i - distance in devices]
    return lax.ppermute(block, axis, route)


def core_groups(size):
    return [[core + CORES * y for y in range(size // CORES)] for core in range(CORES)]


def swap_cores(x):
    size = lax.axis_size("tp")
    return lax.ppermute(x, "tp", [(i, i ^ 1) for i in range(size)])


def minus_expm1(x):
    series = 1.0 + x * (1.0 / 7.0)
    for k in (6, 5, 4, 3, 2):
        series = 1.0 + x * (1.0 / k) * series
    return jnp.where(x > -0.35, -x * series, 1.0 - jnp.exp(x))


def recurrence_kernel(
    x_ref, rim_ref, filter_ref, recur_ref, input_ref, raw_ref, boost_ref,
    state_ref, running_ref, total_ref, ext, decay, drive, gates,
):
    tokens, channels = x_ref.shape
    taps = filter_ref.shape[0]
    blocks, wide, _ = recur_ref.shape
    gates[...] = jnp.zeros_like(gates)
    for at, matrix in ((0, recur_ref), (channels, input_ref)):
        for k in range(blocks):
            low = k * wide
            gates[low : low + wide, at + low : at + low + wide] = matrix[k]
    lead = 8
    ext[lead - taps + 1 : lead, :] = rim_ref[...].astype(jnp.float32)
    ext[lead : lead + tokens, :] = x_ref[...].astype(jnp.float32)
    first = lead - taps + 1
    mixed = ext[first : first + tokens, :] * filter_ref[0:1, :]
    for k in range(1, taps):
        mixed = mixed + ext[first + k : first + k + tokens, :] * filter_ref[k : k + 1, :]
    smoothed = mixed.astype(jnp.bfloat16)
    logits = jnp.dot(smoothed, gates[...], preferred_element_type=jnp.float32)
    both = jax.nn.sigmoid(logits)
    minus_raw = -raw_ref[...]
    soft = jnp.maximum(minus_raw, 0.0) + jnp.log1p(jnp.exp(-jnp.abs(minus_raw)))
    log_decay = both[:, :channels] * (-RECURRENT_SCALE * soft) + boost_ref[...]
    decay[...] = jnp.exp(log_decay)
    drive[...] = jnp.sqrt(minus_expm1(2.0 * log_decay)) * (
        both[:, channels:] * smoothed.astype(jnp.float32)
    )
    length = tokens // SEGMENTS

    def step(i, held):
        state, running = held
        rows = pl.ds(i, SEGMENTS, stride=length)
        a, b = decay[rows, :], drive[rows, :]
        state, running = a * state + b, running * a
        state_ref[rows, :] = state
        running_ref[rows, :] = running
        return state, running

    start = (jnp.zeros((SEGMENTS, channels), jnp.float32), jnp.ones((SEGMENTS, channels), jnp.float32))
    state, running = lax.fori_loop(0, length, step, start, unroll=8)
    whole_a, whole_b = running[0:1], state[0:1]
    for k in range(1, SEGMENTS):
        whole_b = running[k : k + 1] * whole_b + state[k : k + 1]
        whole_a = whole_a * running[k : k + 1]
    total_ref[:, 0:1, :] = jnp.broadcast_to(whole_a[None], (total_ref.shape[0], 1, channels))
    total_ref[:, 1:2, :] = jnp.broadcast_to(whole_b[None], (total_ref.shape[0], 1, channels))


def branch_kernel(place_ref, pieces_ref, state_ref, running_ref, gate_ref, out_ref):
    place = place_ref[0]
    devices, _, channels = pieces_ref.shape
    carry = jnp.zeros((1, channels), jnp.float32)
    for k in range(devices):
        piece = pieces_ref[k]
        carry = jnp.where(k < place, piece[0:1] * carry + piece[1:2], carry)
    length = state_ref.shape[0] // SEGMENTS
    for k in range(SEGMENTS):
        rows = slice(k * length, (k + 1) * length)
        state = state_ref[rows, :] + running_ref[rows, :] * carry
        g = gate_ref[rows, :].astype(jnp.float32)
        gelu = 0.5 * g * (1.0 + jnp.tanh(GELU_SCALE * (g + 0.044715 * (g * g * g))))
        out_ref[rows, :] = (gelu * state).astype(jnp.bfloat16)
        carry = state[length - 1 : length, :]


def slots_kernel(routes_ref, column_ref, line_ref):
    rows = routes_ref.shape[0]
    experts = 32
    number = lax.broadcasted_iota(jnp.int32, (rows, experts), 1)
    hot = [(routes_ref[:, k : k + 1] == number).astype(jnp.float32) for k in range(2)]
    earlier = (
        lax.broadcasted_iota(jnp.int32, (rows, rows), 1)
        < lax.broadcasted_iota(jnp.int32, (rows, rows), 0)
    ).astype(jnp.float32)
    before = jnp.dot(earlier, hot[0] + hot[1], preferred_element_type=jnp.float32)
    wide = line_ref.shape[1]
    lane = lax.broadcasted_iota(jnp.int32, (rows, wide), 1)
    same = lane % rows == lax.broadcasted_iota(jnp.int32, (rows, wide), 0)
    for k in range(2):
        rank = jnp.sum(before * hot[k], axis=1, keepdims=True).astype(jnp.int32)
        slot = routes_ref[:, k : k + 1] * CAP + rank
        column_ref[k * rows : (k + 1) * rows, :] = slot * PIECES
        spread = jnp.where(same, (slot * PIECES).astype(jnp.float32), 0.0)
        line_ref[k : k + 1, :] = (
            jnp.sum(spread, axis=0, keepdims=True).astype(jnp.int32) + lane[0:1] // rows
        )


def mix_kernel(
    branch_ref, weight_ref, resid_ref, gain_ref, line_ref, stream_ref, out_ref, total
):
    step = pl.program_id(0)
    branch = jnp.concatenate([branch_ref[k] for k in range(branch_ref.shape[0])], axis=1)
    term = jnp.dot(branch, weight_ref[...], preferred_element_type=jnp.float32)

    @pl.when(step == 0)
    def _():
        total[...] = term

    @pl.when(step > 0)
    def _():
        total[...] += term

    @pl.when(step == pl.num_programs(0) - 1)
    def _():
        rows, width = resid_ref.shape
        stream = (resid_ref[...].astype(jnp.float32) + total[...]).astype(jnp.bfloat16)
        stream_ref[...] = stream
        wide = stream.astype(jnp.float32)
        mean = jnp.sum(wide * wide, axis=1, keepdims=True) * (1.0 / width)
        normed = (wide * lax.rsqrt(mean + EPSILON) * gain_ref[...]).astype(jnp.bfloat16)
        piece = width // PIECES
        stacked = jnp.concatenate(
            [normed[:, k * piece : (k + 1) * piece] for k in range(PIECES)], axis=0
        )
        spot = lax.broadcasted_iota(jnp.int32, (out_ref.shape[0], rows * PIECES), 0)
        pick = (line_ref[0:1, :] == spot) | (line_ref[1:2, :] == spot)
        pick = pick.astype(jnp.float32).astype(jnp.bfloat16)
        out_ref[...] = jnp.dot(pick, stacked, preferred_element_type=jnp.float32).astype(
            jnp.bfloat16
        )


def expert_kernel(rows_ref, gate_ref, up_ref, down_ref, out_ref):
    rows = rows_ref[...]
    gate = jnp.dot(rows, gate_ref[...], preferred_element_type=jnp.float32)
    upward = jnp.dot(rows, up_ref[...], preferred_element_type=jnp.float32)
    active = (jax.nn.silu(gate) * upward).astype(jnp.bfloat16)
    out_ref[...] = jnp.dot(active, down_ref[...], preferred_element_type=jnp.float32).astype(
        jnp.bfloat16
    )


def combine_kernel(stream_ref, returned_ref, column_ref, weight_ref, out_ref):
    rows, width = stream_ref.shape
    piece = width // PIECES
    spot = lax.broadcasted_iota(jnp.int32, (2 * rows, returned_ref.shape[0]), 1)
    for k in range(PIECES):
        pick = (column_ref[...] + k == spot).astype(jnp.float32).astype(jnp.bfloat16)
        chosen = jnp.dot(pick, returned_ref[...], preferred_element_type=jnp.float32)
        lanes = slice(k * piece, (k + 1) * piece)
        total = weight_ref[:, 0:1] * chosen[:rows] + weight_ref[:, 1:2] * chosen[rows:]
        out_ref[:, lanes] = (stream_ref[:, lanes].astype(jnp.float32) + total).astype(jnp.bfloat16)


def natural(own, other, core, axis):
    return jnp.where(
        core == 0,
        jnp.concatenate([own, other], axis=axis),
        jnp.concatenate([other, own], axis=axis),
    )


def layer(
    resid,
    recurrent_input,
    recurrent_out_gate,
    filter_weight,
    recurrence_gate_matrix,
    input_gate_matrix,
    channel_decay_raw,
    token_decay_boost,
    output_projection_weight,
    expert_norm_gain,
    routes,
    expert_pair_weight,
    gate_weight,
    up_weight,
    down_weight,
):
    tokens, channels = recurrent_input.shape
    taps = filter_weight.shape[0]
    tp, experts = lax.axis_size("tp"), lax.axis_size("sp")
    here, place = lax.axis_index("tp"), lax.axis_index("sp")
    core = here % CORES
    chips = tp // CORES
    groups = core_groups(tp)
    rows_dev, width = resid.shape
    f32, bf16 = jnp.float32, jnp.bfloat16

    rim = shifted(recurrent_input[tokens - taps + 1 :], "sp", 1)
    projection = lax.all_gather(output_projection_weight, "tp", axis=0, tiled=True)

    own_routes = lax.dynamic_slice_in_dim(routes, here * rows_dev, rows_dev, 0)
    column, line = pl.pallas_call(
        slots_kernel,
        out_shape=(
            jax.ShapeDtypeStruct((2 * rows_dev, 1), jnp.int32),
            jax.ShapeDtypeStruct((2, PIECES * rows_dev), jnp.int32),
        ),
        in_specs=[VMEM],
        out_specs=(VMEM,) * 2,
        name="slots",
    )(own_routes)

    state, running, total = pl.pallas_call(
        recurrence_kernel,
        out_shape=(
            jax.ShapeDtypeStruct((tokens, channels), f32),
            jax.ShapeDtypeStruct((tokens, channels), f32),
            jax.ShapeDtypeStruct((experts, 2, channels), f32),
        ),
        in_specs=[VMEM] * 7,
        out_specs=(VMEM,) * 3,
        scratch_shapes=[
            pltpu.VMEM((tokens + 8, channels), f32),
            pltpu.VMEM((tokens, channels), f32),
            pltpu.VMEM((tokens, channels), f32),
            pltpu.VMEM((channels, 2 * channels), bf16),
        ],
        cost_estimate=pl.CostEstimate(flops=10**9, bytes_accessed=2**20, transcendentals=0),
        name="recurrence",
    )(
        recurrent_input,
        rim,
        filter_weight,
        recurrence_gate_matrix,
        input_gate_matrix,
        channel_decay_raw[None, :],
        token_decay_boost,
    )

    pieces = lax.all_to_all(total, "sp", 0, 0, tiled=True)
    branch = pl.pallas_call(
        branch_kernel,
        out_shape=jax.ShapeDtypeStruct((tokens, channels), bf16),
        in_specs=[SMEM] + [VMEM] * 4,
        out_specs=VMEM,
        name="branch",
    )(place.astype(jnp.int32)[None], pieces, state, running, recurrent_out_gate)
    mine = lax.all_to_all(branch.reshape(tp, rows_dev, channels), "tp", 0, 0, tiled=True)

    slot_count = experts * CAP
    depth = CORES * channels
    whole = lambda *shape: pl.BlockSpec(shape, lambda k: (0,) * len(shape))
    stream, outgoing = pl.pallas_call(
        mix_kernel,
        grid=(chips,),
        out_shape=(
            jax.ShapeDtypeStruct((rows_dev, width), bf16),
            jax.ShapeDtypeStruct((slot_count * PIECES, width // PIECES), bf16),
        ),
        in_specs=[
            pl.BlockSpec((CORES, rows_dev, channels), lambda k: (k, 0, 0)),
            pl.BlockSpec((depth, width), lambda k: (k, 0)),
            whole(rows_dev, width),
            whole(1, width),
            whole(2, PIECES * rows_dev),
        ],
        out_specs=(
            whole(rows_dev, width),
            whole(slot_count * PIECES, width // PIECES),
        ),
        scratch_shapes=[pltpu.VMEM((rows_dev, width), f32)],
        name="mix",
    )(mine, projection, resid, expert_norm_gain[None, :], line)
    packed = (experts, CAP * PIECES, width // PIECES)
    arrived = lax.all_to_all(outgoing.reshape(packed), "sp", 0, 0, tiled=True)
    arrived = arrived.reshape(slot_count, width)

    rows = lax.all_gather(arrived, "tp", axis=0, axis_index_groups=groups, tiled=True)
    arrived, down_part, gate_own, up_own = lax.optimization_barrier(
        (arrived, down_weight[0], gate_weight[0], up_weight[0])
    )
    hidden = gate_own.shape[1]
    down_own = lax.all_to_all(
        down_part.reshape(chips, CORES * hidden, -1), "tp", 0, 0,
        axis_index_groups=groups, tiled=True,
    )
    gate = natural(gate_own, swap_cores(gate_own), core, 1)
    upward = natural(up_own, swap_cores(up_own), core, 1)
    down = natural(down_own[:, None], swap_cores(down_own)[:, None], core, 1)
    down = jnp.moveaxis(down.reshape(tp, CORES * hidden, -1), 0, 1).reshape(CORES * hidden, width)
    depth = CORES * hidden
    block = rows.shape[0] // 4
    summed = pl.pallas_call(
        expert_kernel,
        grid=(4,),
        out_shape=jax.ShapeDtypeStruct(rows.shape, bf16),
        in_specs=[
            pl.BlockSpec((block, width), lambda k: (k, 0)),
            whole(width, depth),
            whole(width, depth),
            whole(depth, width),
        ],
        out_specs=pl.BlockSpec((block, width), lambda k: (k, 0)),
        name="experts",
    )(rows, gate, upward, down)
    result = lax.psum_scatter(
        summed, "tp", scatter_dimension=0, axis_index_groups=groups, tiled=True
    )

    returned = lax.all_to_all(result.reshape(packed), "sp", 0, 0, tiled=True)
    return pl.pallas_call(
        combine_kernel,
        out_shape=jax.ShapeDtypeStruct((rows_dev, width), bf16),
        in_specs=[VMEM] * 4,
        out_specs=VMEM,
        name="combine",
    )(stream, returned.reshape(slot_count * PIECES, width // PIECES), column, expert_pair_weight)


def solution(mesh):
    placed = (
        P(("sp", "tp"), None),
        P("sp", "tp"),
        P("sp", "tp"),
        P(None, "tp"),
        P("tp", None, None),
        P("tp", None, None),
        P("tp"),
        P("sp", "tp"),
        P("tp", None),
        P(),
        P("sp", None),
        P(("sp", "tp"), None),
        P("sp", None, "tp"),
        P("sp", None, "tp"),
        P("sp", None, "tp"),
    )
    return jax.shard_map(
        layer, mesh=mesh, in_specs=placed, out_specs=P(("sp", "tp"), None), check_vma=False
    )
```

```python
import jax
import jax.numpy as jnp
from jax import lax
from jax.experimental import pallas as pl
from jax.experimental.pallas import tpu as pltpu
from jax.sharding import PartitionSpec as P


RECURRENT_SCALE = 8.0
EPSILON = 1e-06
SEGMENTS = 8
CORES = 2
CAP = 3
PIECES = 8
INNER = 4
GELU_SCALE = 0.7978845608028654

VMEM = pl.BlockSpec(memory_space=pltpu.VMEM)
SMEM = pl.BlockSpec(memory_space=pltpu.SMEM)


def shifted(block, axis, distance):
    devices = range(lax.axis_size(axis))
    route = [(i - distance, i) for i in devices if i - distance in devices]
    return lax.ppermute(block, axis, route)


def core_groups(size):
    return [[core + CORES * y for y in range(size // CORES)] for core in range(CORES)]


def halves_of_chips(size):
    return [[i for i in range(size) if i // CORES % 2 == side] for side in range(2)]


def swap_neighbours(x):
    size = lax.axis_size("tp")
    return lax.ppermute(x, "tp", [(i, i ^ CORES) for i in range(size)])


def swap_cores(x):
    size = lax.axis_size("tp")
    return lax.ppermute(x, "tp", [(i, i ^ 1) for i in range(size)])


def minus_expm1(x):
    series = 1.0 + x * (1.0 / 7.0)
    for k in (6, 5, 4, 3, 2):
        series = 1.0 + x * (1.0 / k) * series
    return jnp.where(x > -0.35, -x * series, 1.0 - jnp.exp(x))


def recurrence_kernel(
    x_ref, rim_ref, filter_ref, recur_ref, input_ref, raw_ref, boost_ref,
    state_ref, running_ref, total_ref, ext, decay, drive, gates,
):
    tokens, channels = x_ref.shape
    taps = filter_ref.shape[0]
    blocks, wide, _ = recur_ref.shape
    gates[...] = jnp.zeros_like(gates)
    for at, matrix in ((0, recur_ref), (channels, input_ref)):
        for k in range(blocks):
            low = k * wide
            gates[low : low + wide, at + low : at + low + wide] = matrix[k]
    lead = 8
    ext[lead - taps + 1 : lead, :] = rim_ref[...].astype(jnp.float32)
    ext[lead : lead + tokens, :] = x_ref[...].astype(jnp.float32)
    first = lead - taps + 1
    mixed = ext[first : first + tokens, :] * filter_ref[0:1, :]
    for k in range(1, taps):
        mixed = mixed + ext[first + k : first + k + tokens, :] * filter_ref[k : k + 1, :]
    smoothed = mixed.astype(jnp.bfloat16)
    logits = jnp.dot(smoothed, gates[...], preferred_element_type=jnp.float32)
    both = jax.nn.sigmoid(logits)
    minus_raw = -raw_ref[...]
    soft = jnp.maximum(minus_raw, 0.0) + jnp.log1p(jnp.exp(-jnp.abs(minus_raw)))
    log_decay = both[:, :channels] * (-RECURRENT_SCALE * soft) + boost_ref[...]
    decay[...] = jnp.exp(log_decay)
    drive[...] = jnp.sqrt(minus_expm1(2.0 * log_decay)) * (
        both[:, channels:] * smoothed.astype(jnp.float32)
    )
    length = tokens // SEGMENTS

    def step(i, held):
        state, running = held
        rows = pl.ds(i, SEGMENTS, stride=length)
        a, b = decay[rows, :], drive[rows, :]
        state, running = a * state + b, running * a
        state_ref[rows, :] = state
        running_ref[rows, :] = running
        return state, running

    start = (jnp.zeros((SEGMENTS, channels), jnp.float32), jnp.ones((SEGMENTS, channels), jnp.float32))
    state, running = lax.fori_loop(0, length, step, start, unroll=8)
    whole_a, whole_b = running[0:1], state[0:1]
    for k in range(1, SEGMENTS):
        whole_b = running[k : k + 1] * whole_b + state[k : k + 1]
        whole_a = whole_a * running[k : k + 1]
    total_ref[:, 0:1, :] = jnp.broadcast_to(whole_a[None], (total_ref.shape[0], 1, channels))
    total_ref[:, 1:2, :] = jnp.broadcast_to(whole_b[None], (total_ref.shape[0], 1, channels))


def inner_kernel(pieces_ref, total_ref):
    count, _, channels = pieces_ref.shape
    whole_a, whole_b = pieces_ref[0, 0:1, :], pieces_ref[0, 1:2, :]
    for k in range(1, count):
        a, b = pieces_ref[k, 0:1, :], pieces_ref[k, 1:2, :]
        whole_b = a * whole_b + b
        whole_a = whole_a * a
    total_ref[:, 0:1, :] = jnp.broadcast_to(whole_a[None], (total_ref.shape[0], 1, channels))
    total_ref[:, 1:2, :] = jnp.broadcast_to(whole_b[None], (total_ref.shape[0], 1, channels))


def branch_kernel(place_ref, outer_ref, inner_ref, state_ref, running_ref, gate_ref, out_ref):
    carry = jnp.zeros((1, state_ref.shape[1]), jnp.float32)
    for place, pieces in ((place_ref[0], outer_ref), (place_ref[1], inner_ref)):
        for k in range(pieces.shape[0]):
            after = pieces[k, 0:1, :] * carry + pieces[k, 1:2, :]
            carry = jnp.where(k < place, after, carry)
    length = state_ref.shape[0] // SEGMENTS
    half = length // CORES
    for k in range(SEGMENTS):
        rows = slice(k * length, (k + 1) * length)
        state = state_ref[rows, :] + running_ref[rows, :] * carry
        g = gate_ref[rows, :].astype(jnp.float32)
        gelu = 0.5 * g * (1.0 + jnp.tanh(GELU_SCALE * (g + 0.044715 * (g * g * g))))
        branch = (gelu * state).astype(jnp.bfloat16)
        for core in range(CORES):
            out_ref[k // 2 * CORES + core, k % 2 * half : (k % 2 + 1) * half, :] = branch[
                core * half : (core + 1) * half
            ]
        carry = state[length - 1 : length, :]


def slots_kernel(routes_ref, column_ref, line_ref):
    rows = routes_ref.shape[0]
    experts = 32
    number = lax.broadcasted_iota(jnp.int32, (rows, experts), 1)
    hot = [(routes_ref[:, k : k + 1] == number).astype(jnp.float32) for k in range(2)]
    earlier = (
        lax.broadcasted_iota(jnp.int32, (rows, rows), 1)
        < lax.broadcasted_iota(jnp.int32, (rows, rows), 0)
    ).astype(jnp.float32)
    before = jnp.dot(earlier, hot[0] + hot[1], preferred_element_type=jnp.float32)
    wide = line_ref.shape[1]
    lane = lax.broadcasted_iota(jnp.int32, (rows, wide), 1)
    same = lane % rows == lax.broadcasted_iota(jnp.int32, (rows, wide), 0)
    for k in range(2):
        rank = jnp.sum(before * hot[k], axis=1, keepdims=True).astype(jnp.int32)
        slot = routes_ref[:, k : k + 1] * CAP + rank
        column_ref[k * rows : (k + 1) * rows, :] = slot * PIECES
        spread = jnp.where(same, (slot * PIECES).astype(jnp.float32), 0.0)
        line_ref[k : k + 1, :] = (
            jnp.sum(spread, axis=0, keepdims=True).astype(jnp.int32) + lane[0:1] // rows
        )


def project_kernel(side_ref, branch_ref, weight_ref, keep_ref, send_ref, total):
    step = pl.program_id(0)
    branch = jnp.concatenate([branch_ref[k] for k in range(branch_ref.shape[0])], axis=1)
    term = jnp.dot(branch, weight_ref[...], preferred_element_type=jnp.float32)

    @pl.when(step == 0)
    def _():
        total[...] = term

    @pl.when(step > 0)
    def _():
        total[...] += term

    @pl.when(step == pl.num_programs(0) - 1)
    def _():
        side, rows = side_ref[0], keep_ref.shape[0]
        keep_ref[...] = total[pl.ds(pl.multiple_of(side * rows, rows), rows), :]
        other = pl.ds(pl.multiple_of((1 - side) * rows, rows), rows)
        send_ref[...] = total[other, :].astype(jnp.bfloat16)


def dispatch_kernel(keep_ref, got_ref, resid_ref, gain_ref, line_ref, stream_ref, out_ref):
    rows, width = resid_ref.shape
    projected = keep_ref[...] + got_ref[...].astype(jnp.float32)
    stream = (resid_ref[...].astype(jnp.float32) + projected).astype(jnp.bfloat16)
    stream_ref[...] = stream
    wide = stream.astype(jnp.float32)
    mean = jnp.sum(wide * wide, axis=1, keepdims=True) * (1.0 / width)
    normed = (wide * lax.rsqrt(mean + EPSILON) * gain_ref[...]).astype(jnp.bfloat16)
    piece = width // PIECES
    stacked = jnp.concatenate(
        [normed[:, k * piece : (k + 1) * piece] for k in range(PIECES)], axis=0
    )
    spot = lax.broadcasted_iota(jnp.int32, (out_ref.shape[0], rows * PIECES), 0)
    pick = (line_ref[0:1, :] == spot) | (line_ref[1:2, :] == spot)
    pick = pick.astype(jnp.float32).astype(jnp.bfloat16)
    out_ref[...] = jnp.dot(pick, stacked, preferred_element_type=jnp.float32).astype(jnp.bfloat16)


def expert_kernel(rows_ref, gate_ref, up_ref, down_ref, out_ref):
    rows = rows_ref[...]
    gate = jnp.dot(rows, gate_ref[...], preferred_element_type=jnp.float32)
    upward = jnp.dot(rows, up_ref[...], preferred_element_type=jnp.float32)
    active = (jax.nn.silu(gate) * upward).astype(jnp.bfloat16)
    out_ref[...] = jnp.dot(active, down_ref[...], preferred_element_type=jnp.float32).astype(
        jnp.bfloat16
    )


def combine_kernel(stream_ref, returned_ref, column_ref, weight_ref, out_ref):
    rows, width = stream_ref.shape
    piece = width // PIECES
    spot = lax.broadcasted_iota(jnp.int32, (2 * rows, returned_ref.shape[0]), 1)
    for k in range(PIECES):
        pick = (column_ref[...] + k == spot).astype(jnp.float32).astype(jnp.bfloat16)
        chosen = jnp.dot(pick, returned_ref[...], preferred_element_type=jnp.float32)
        lanes = slice(k * piece, (k + 1) * piece)
        total = weight_ref[:, 0:1] * chosen[:rows] + weight_ref[:, 1:2] * chosen[rows:]
        out_ref[:, lanes] = (stream_ref[:, lanes].astype(jnp.float32) + total).astype(jnp.bfloat16)


def natural(own, other, core, axis):
    return jnp.where(
        core == 0,
        jnp.concatenate([own, other], axis=axis),
        jnp.concatenate([other, own], axis=axis),
    )


def layer(
    resid,
    recurrent_input,
    recurrent_out_gate,
    filter_weight,
    recurrence_gate_matrix,
    input_gate_matrix,
    channel_decay_raw,
    token_decay_boost,
    output_projection_weight,
    expert_norm_gain,
    routes,
    expert_pair_weight,
    gate_weight,
    up_weight,
    down_weight,
):
    tokens, channels = recurrent_input.shape
    taps = filter_weight.shape[0]
    tp, experts = lax.axis_size("tp"), lax.axis_size("sp")
    here, place = lax.axis_index("tp"), lax.axis_index("sp")
    core = here % CORES
    chips = tp // CORES
    groups, halves = core_groups(tp), halves_of_chips(tp)
    side = here // CORES % 2
    outer = experts // INNER
    inner_groups = [[k * INNER + i for i in range(INNER)] for k in range(outer)]
    outer_groups = [[k * INNER + i for k in range(outer)] for i in range(INNER)]
    rows_dev, width = resid.shape
    f32, bf16 = jnp.float32, jnp.bfloat16

    rim = shifted(recurrent_input[tokens - taps + 1 :], "sp", 1)
    projection = lax.all_gather(
        output_projection_weight, "tp", axis=0, axis_index_groups=halves, tiled=True
    )

    own_routes = lax.dynamic_slice_in_dim(routes, here * rows_dev, rows_dev, 0)
    column, line = pl.pallas_call(
        slots_kernel,
        out_shape=(
            jax.ShapeDtypeStruct((2 * rows_dev, 1), jnp.int32),
            jax.ShapeDtypeStruct((2, PIECES * rows_dev), jnp.int32),
        ),
        in_specs=[VMEM],
        out_specs=(VMEM,) * 2,
        name="slots",
    )(own_routes)

    state, running, total = pl.pallas_call(
        recurrence_kernel,
        out_shape=(
            jax.ShapeDtypeStruct((tokens, channels), f32),
            jax.ShapeDtypeStruct((tokens, channels), f32),
            jax.ShapeDtypeStruct((INNER, 2, channels), f32),
        ),
        in_specs=[VMEM] * 7,
        out_specs=(VMEM,) * 3,
        scratch_shapes=[
            pltpu.VMEM((tokens + 8, channels), f32),
            pltpu.VMEM((tokens, channels), f32),
            pltpu.VMEM((tokens, channels), f32),
            pltpu.VMEM((channels, 2 * channels), bf16),
        ],
        cost_estimate=pl.CostEstimate(flops=10**9, bytes_accessed=2**20, transcendentals=0),
        name="recurrence",
    )(
        recurrent_input,
        rim,
        filter_weight,
        recurrence_gate_matrix,
        input_gate_matrix,
        channel_decay_raw[None, :],
        token_decay_boost,
    )

    inner_pieces = lax.all_to_all(
        total, "sp", 0, 0, axis_index_groups=inner_groups, tiled=True
    )
    total = pl.pallas_call(
        inner_kernel,
        out_shape=jax.ShapeDtypeStruct((outer, 2, channels), f32),
        in_specs=[VMEM],
        out_specs=VMEM,
        name="inner",
    )(inner_pieces)
    outer_pieces = lax.all_to_all(
        total, "sp", 0, 0, axis_index_groups=outer_groups, tiled=True
    )
    peers = tp // 2
    branch = pl.pallas_call(
        branch_kernel,
        out_shape=jax.ShapeDtypeStruct((peers, 2 * rows_dev, channels), bf16),
        in_specs=[SMEM] + [VMEM] * 5,
        out_specs=VMEM,
        name="branch",
    )(
        jnp.stack([place // INNER, place % INNER]).astype(jnp.int32),
        outer_pieces, inner_pieces, state, running, recurrent_out_gate,
    )
    mine = lax.all_to_all(branch, "tp", 0, 0, axis_index_groups=halves, tiled=True)

    slot_count = experts * CAP
    depth = CORES * channels
    whole = lambda *shape: pl.BlockSpec(shape, lambda k: (0,) * len(shape))
    keep, send = pl.pallas_call(
        project_kernel,
        grid=(peers // CORES,),
        out_shape=(
            jax.ShapeDtypeStruct((rows_dev, width), f32),
            jax.ShapeDtypeStruct((rows_dev, width), bf16),
        ),
        in_specs=[
            SMEM,
            pl.BlockSpec((CORES, 2 * rows_dev, channels), lambda k: (k, 0, 0)),
            pl.BlockSpec((depth, width), lambda k: (k, 0)),
        ],
        out_specs=(whole(rows_dev, width),) * 2,
        scratch_shapes=[pltpu.VMEM((2 * rows_dev, width), f32)],
        name="project",
    )(side.astype(jnp.int32)[None], mine, projection)
    got = swap_neighbours(send)
    stream, outgoing = pl.pallas_call(
        dispatch_kernel,
        out_shape=(
            jax.ShapeDtypeStruct((rows_dev, width), bf16),
            jax.ShapeDtypeStruct((slot_count * PIECES, width // PIECES), bf16),
        ),
        in_specs=[VMEM] * 5,
        out_specs=(VMEM,) * 2,
        name="dispatch",
    )(keep, got, resid, expert_norm_gain[None, :], line)
    packed = (experts, CAP * PIECES, width // PIECES)
    arrived = lax.all_to_all(outgoing.reshape(packed), "sp", 0, 0, tiled=True)
    arrived = arrived.reshape(slot_count, width)

    rows = lax.all_gather(arrived, "tp", axis=0, axis_index_groups=groups, tiled=True)
    arrived, down_part, gate_own, up_own = lax.optimization_barrier(
        (arrived, down_weight[0], gate_weight[0], up_weight[0])
    )
    hidden = gate_own.shape[1]
    down_own = lax.all_to_all(
        down_part.reshape(chips, CORES * hidden, -1), "tp", 0, 0,
        axis_index_groups=groups, tiled=True,
    )
    gate = natural(gate_own, swap_cores(gate_own), core, 1)
    upward = natural(up_own, swap_cores(up_own), core, 1)
    down = natural(down_own[:, None], swap_cores(down_own)[:, None], core, 1)
    down = jnp.moveaxis(down.reshape(tp, CORES * hidden, -1), 0, 1).reshape(CORES * hidden, width)
    depth = CORES * hidden
    block = rows.shape[0] // 4
    summed = pl.pallas_call(
        expert_kernel,
        grid=(4,),
        out_shape=jax.ShapeDtypeStruct(rows.shape, bf16),
        in_specs=[
            pl.BlockSpec((block, width), lambda k: (k, 0)),
            whole(width, depth),
            whole(width, depth),
            whole(depth, width),
        ],
        out_specs=pl.BlockSpec((block, width), lambda k: (k, 0)),
        name="experts",
    )(rows, gate, upward, down)
    result = lax.psum_scatter(
        summed, "tp", scatter_dimension=0, axis_index_groups=groups, tiled=True
    )

    returned = lax.all_to_all(result.reshape(packed), "sp", 0, 0, tiled=True)
    return pl.pallas_call(
        combine_kernel,
        out_shape=jax.ShapeDtypeStruct((rows_dev, width), bf16),
        in_specs=[VMEM] * 4,
        out_specs=VMEM,
        name="combine",
    )(stream, returned.reshape(slot_count * PIECES, width // PIECES), column, expert_pair_weight)


def solution(mesh):
    placed = (
        P(("sp", "tp"), None),
        P("sp", "tp"),
        P("sp", "tp"),
        P(None, "tp"),
        P("tp", None, None),
        P("tp", None, None),
        P("tp"),
        P("sp", "tp"),
        P("tp", None),
        P(),
        P("sp", None),
        P(("sp", "tp"), None),
        P("sp", None, "tp"),
        P("sp", None, "tp"),
        P("sp", None, "tp"),
    )
    return jax.shard_map(
        layer, mesh=mesh, in_specs=placed, out_specs=P(("sp", "tp"), None), check_vma=False
    )
```

```python
import jax
import jax.numpy as jnp
from jax import lax
from jax.experimental import pallas as pl
from jax.experimental.pallas import tpu as pltpu
from jax.sharding import PartitionSpec as P


RECURRENT_SCALE = 8.0
EPSILON = 1e-06
SEGMENTS = 8
CORES = 2
CAP = 3
PIECES = 8
GELU_SCALE = 0.7978845608028654

VMEM = pl.BlockSpec(memory_space=pltpu.VMEM)
SMEM = pl.BlockSpec(memory_space=pltpu.SMEM)


def shifted(block, axis, distance):
    devices = range(lax.axis_size(axis))
    route = [(i - distance, i) for i in devices if i - distance in devices]
    return lax.ppermute(block, axis, route)


def core_groups(size):
    return [[core + CORES * y for y in range(size // CORES)] for core in range(CORES)]


def swap_cores(x):
    size = lax.axis_size("tp")
    return lax.ppermute(x, "tp", [(i, i ^ 1) for i in range(size)])


def minus_expm1(x):
    series = 1.0 + x * (1.0 / 7.0)
    for k in (6, 5, 4, 3, 2):
        series = 1.0 + x * (1.0 / k) * series
    return jnp.where(x > -0.35, -x * series, 1.0 - jnp.exp(x))


def recurrence_kernel(
    x_ref, rim_ref, filter_ref, recur_ref, input_ref, raw_ref, boost_ref,
    state_ref, running_ref, total_ref, ext, decay, drive, gates,
):
    tokens, channels = x_ref.shape
    taps = filter_ref.shape[0]
    blocks, wide, _ = recur_ref.shape
    gates[...] = jnp.zeros_like(gates)
    for at, matrix in ((0, recur_ref), (channels, input_ref)):
        for k in range(blocks):
            low = k * wide
            gates[low : low + wide, at + low : at + low + wide] = matrix[k]
    lead = 8
    ext[lead - taps + 1 : lead, :] = rim_ref[...].astype(jnp.float32)
    ext[lead : lead + tokens, :] = x_ref[...].astype(jnp.float32)
    first = lead - taps + 1
    mixed = ext[first : first + tokens, :] * filter_ref[0:1, :]
    for k in range(1, taps):
        mixed = mixed + ext[first + k : first + k + tokens, :] * filter_ref[k : k + 1, :]
    smoothed = mixed.astype(jnp.bfloat16)
    logits = jnp.dot(smoothed, gates[...], preferred_element_type=jnp.float32)
    both = jax.nn.sigmoid(logits)
    minus_raw = -raw_ref[...]
    soft = jnp.maximum(minus_raw, 0.0) + jnp.log1p(jnp.exp(-jnp.abs(minus_raw)))
    log_decay = both[:, :channels] * (-RECURRENT_SCALE * soft) + boost_ref[...]
    decay[...] = jnp.exp(log_decay)
    drive[...] = jnp.sqrt(minus_expm1(2.0 * log_decay)) * (
        both[:, channels:] * smoothed.astype(jnp.float32)
    )
    length = tokens // SEGMENTS

    def step(i, held):
        state, running = held
        rows = pl.ds(i, SEGMENTS, stride=length)
        a, b = decay[rows, :], drive[rows, :]
        state, running = a * state + b, running * a
        state_ref[rows, :] = state
        running_ref[rows, :] = running
        return state, running

    start = (jnp.zeros((SEGMENTS, channels), jnp.float32), jnp.ones((SEGMENTS, channels), jnp.float32))
    state, running = lax.fori_loop(0, length, step, start, unroll=8)
    whole_a, whole_b = running[0:1], state[0:1]
    for k in range(1, SEGMENTS):
        whole_b = running[k : k + 1] * whole_b + state[k : k + 1]
        whole_a = whole_a * running[k : k + 1]
    total_ref[:, 0:1, :] = jnp.broadcast_to(whole_a[None], (total_ref.shape[0], 1, channels))
    total_ref[:, 1:2, :] = jnp.broadcast_to(whole_b[None], (total_ref.shape[0], 1, channels))


def branch_kernel(place_ref, pieces_ref, state_ref, running_ref, gate_ref, out_ref):
    place = place_ref[0]
    carry = jnp.zeros((1, state_ref.shape[1]), jnp.float32)
    for k in range(pieces_ref.shape[0]):
        after = pieces_ref[k, 0:1, :] * carry + pieces_ref[k, 1:2, :]
        carry = jnp.where(k < place, after, carry)
    length = state_ref.shape[0] // SEGMENTS
    for k in range(SEGMENTS):
        rows = slice(k * length, (k + 1) * length)
        state = state_ref[rows, :] + running_ref[rows, :] * carry
        g = gate_ref[rows, :].astype(jnp.float32)
        gelu = 0.5 * g * (1.0 + jnp.tanh(GELU_SCALE * (g + 0.044715 * (g * g * g))))
        out_ref[rows, :] = (gelu * state).astype(jnp.bfloat16)
        carry = state[length - 1 : length, :]


def slots_kernel(routes_ref, column_ref, line_ref):
    rows = routes_ref.shape[0]
    experts = 32
    number = lax.broadcasted_iota(jnp.int32, (rows, experts), 1)
    hot = [(routes_ref[:, k : k + 1] == number).astype(jnp.float32) for k in range(2)]
    earlier = (
        lax.broadcasted_iota(jnp.int32, (rows, rows), 1)
        < lax.broadcasted_iota(jnp.int32, (rows, rows), 0)
    ).astype(jnp.float32)
    before = jnp.dot(earlier, hot[0] + hot[1], preferred_element_type=jnp.float32)
    wide = line_ref.shape[1]
    lane = lax.broadcasted_iota(jnp.int32, (rows, wide), 1)
    same = lane % rows == lax.broadcasted_iota(jnp.int32, (rows, wide), 0)
    for k in range(2):
        rank = jnp.sum(before * hot[k], axis=1, keepdims=True).astype(jnp.int32)
        slot = routes_ref[:, k : k + 1] * CAP + rank
        column_ref[k * rows : (k + 1) * rows, :] = slot * PIECES
        spread = jnp.where(same, (slot * PIECES).astype(jnp.float32), 0.0)
        line_ref[k : k + 1, :] = (
            jnp.sum(spread, axis=0, keepdims=True).astype(jnp.int32) + lane[0:1] // rows
        )


def project_kernel(side_ref, branch_ref, weight_ref, keep_ref, send_ref, total):
    step = pl.program_id(0)
    branch = jnp.concatenate([branch_ref[k] for k in range(branch_ref.shape[0])], axis=1)
    term = jnp.dot(branch, weight_ref[...], preferred_element_type=jnp.float32)

    @pl.when(step == 0)
    def _():
        total[...] = term

    @pl.when(step > 0)
    def _():
        total[...] += term

    @pl.when(step == pl.num_programs(0) - 1)
    def _():
        side, rows = side_ref[0], keep_ref.shape[0]
        keep_ref[...] = total[pl.ds(pl.multiple_of(side * rows, rows), rows), :]
        other = pl.ds(pl.multiple_of((1 - side) * rows, rows), rows)
        send_ref[...] = total[other, :].astype(jnp.bfloat16)


def dispatch_kernel(keep_ref, got_ref, resid_ref, gain_ref, line_ref, stream_ref, out_ref):
    rows, width = resid_ref.shape
    projected = keep_ref[...] + got_ref[...].astype(jnp.float32)
    stream = (resid_ref[...].astype(jnp.float32) + projected).astype(jnp.bfloat16)
    stream_ref[...] = stream
    wide = stream.astype(jnp.float32)
    mean = jnp.sum(wide * wide, axis=1, keepdims=True) * (1.0 / width)
    normed = (wide * lax.rsqrt(mean + EPSILON) * gain_ref[...]).astype(jnp.bfloat16)
    piece = width // PIECES
    stacked = jnp.concatenate(
        [normed[:, k * piece : (k + 1) * piece] for k in range(PIECES)], axis=0
    )
    spot = lax.broadcasted_iota(jnp.int32, (out_ref.shape[0], rows * PIECES), 0)
    pick = (line_ref[0:1, :] == spot) | (line_ref[1:2, :] == spot)
    pick = pick.astype(jnp.float32).astype(jnp.bfloat16)
    out_ref[...] = jnp.dot(pick, stacked, preferred_element_type=jnp.float32).astype(jnp.bfloat16)


def expert_kernel(rows_ref, gate_ref, up_ref, down_ref, out_ref):
    rows = rows_ref[...]
    gate = jnp.dot(rows, gate_ref[...], preferred_element_type=jnp.float32)
    upward = jnp.dot(rows, up_ref[...], preferred_element_type=jnp.float32)
    active = (jax.nn.silu(gate) * upward).astype(jnp.bfloat16)
    out_ref[...] = jnp.dot(active, down_ref[...], preferred_element_type=jnp.float32).astype(
        jnp.bfloat16
    )


def combine_kernel(stream_ref, returned_ref, column_ref, weight_ref, out_ref):
    rows, width = stream_ref.shape
    piece = width // PIECES
    spot = lax.broadcasted_iota(jnp.int32, (2 * rows, returned_ref.shape[0]), 1)
    for k in range(PIECES):
        pick = (column_ref[...] + k == spot).astype(jnp.float32).astype(jnp.bfloat16)
        chosen = jnp.dot(pick, returned_ref[...], preferred_element_type=jnp.float32)
        lanes = slice(k * piece, (k + 1) * piece)
        total = weight_ref[:, 0:1] * chosen[:rows] + weight_ref[:, 1:2] * chosen[rows:]
        out_ref[:, lanes] = (stream_ref[:, lanes].astype(jnp.float32) + total).astype(jnp.bfloat16)


def natural(own, other, core, axis):
    return jnp.where(
        core == 0,
        jnp.concatenate([own, other], axis=axis),
        jnp.concatenate([other, own], axis=axis),
    )


def layer(
    resid,
    recurrent_input,
    recurrent_out_gate,
    filter_weight,
    recurrence_gate_matrix,
    input_gate_matrix,
    channel_decay_raw,
    token_decay_boost,
    output_projection_weight,
    expert_norm_gain,
    routes,
    expert_pair_weight,
    gate_weight,
    up_weight,
    down_weight,
):
    tokens, channels = recurrent_input.shape
    taps = filter_weight.shape[0]
    tp, experts = lax.axis_size("tp"), lax.axis_size("sp")
    here, place = lax.axis_index("tp"), lax.axis_index("sp")
    core = here % CORES
    chips = tp // CORES
    groups = core_groups(tp)
    rows_dev, width = resid.shape
    f32, bf16 = jnp.float32, jnp.bfloat16

    rim = shifted(recurrent_input[tokens - taps + 1 :], "sp", 1)
    projection = lax.all_gather(
        output_projection_weight, "tp", axis=0, axis_index_groups=groups, tiled=True
    )

    own_routes = lax.dynamic_slice_in_dim(routes, here * rows_dev, rows_dev, 0)
    column, line = pl.pallas_call(
        slots_kernel,
        out_shape=(
            jax.ShapeDtypeStruct((2 * rows_dev, 1), jnp.int32),
            jax.ShapeDtypeStruct((2, PIECES * rows_dev), jnp.int32),
        ),
        in_specs=[VMEM],
        out_specs=(VMEM,) * 2,
        name="slots",
    )(own_routes)

    state, running, total = pl.pallas_call(
        recurrence_kernel,
        out_shape=(
            jax.ShapeDtypeStruct((tokens, channels), f32),
            jax.ShapeDtypeStruct((tokens, channels), f32),
            jax.ShapeDtypeStruct((experts, 2, channels), f32),
        ),
        in_specs=[VMEM] * 7,
        out_specs=(VMEM,) * 3,
        scratch_shapes=[
            pltpu.VMEM((tokens + 8, channels), f32),
            pltpu.VMEM((tokens, channels), f32),
            pltpu.VMEM((tokens, channels), f32),
            pltpu.VMEM((channels, 2 * channels), bf16),
        ],
        cost_estimate=pl.CostEstimate(flops=10**9, bytes_accessed=2**20, transcendentals=0),
        name="recurrence",
    )(
        recurrent_input,
        rim,
        filter_weight,
        recurrence_gate_matrix,
        input_gate_matrix,
        channel_decay_raw[None, :],
        token_decay_boost,
    )

    pieces = lax.all_to_all(total, "sp", 0, 0, tiled=True)
    branch = pl.pallas_call(
        branch_kernel,
        out_shape=jax.ShapeDtypeStruct((tokens, channels), bf16),
        in_specs=[SMEM] + [VMEM] * 4,
        out_specs=VMEM,
        name="branch",
    )(place.astype(jnp.int32)[None], pieces, state, running, recurrent_out_gate)
    mine = lax.all_to_all(
        branch.reshape(chips, CORES * rows_dev, channels), "tp", 0, 0,
        axis_index_groups=groups, tiled=True,
    )
    down_part = lax.optimization_barrier((down_weight[0], mine))[0]
    hidden = gate_weight.shape[2]
    down_own = lax.all_to_all(
        down_part.reshape(chips, CORES * hidden, -1), "tp", 0, 0,
        axis_index_groups=groups, tiled=True,
    )

    slot_count = experts * CAP
    depth = CORES * channels
    whole = lambda *shape: pl.BlockSpec(shape, lambda k: (0,) * len(shape))
    keep, send = pl.pallas_call(
        project_kernel,
        grid=(chips // CORES,),
        out_shape=(
            jax.ShapeDtypeStruct((rows_dev, width), f32),
            jax.ShapeDtypeStruct((rows_dev, width), bf16),
        ),
        in_specs=[
            SMEM,
            pl.BlockSpec((CORES, 2 * rows_dev, channels), lambda k: (k, 0, 0)),
            pl.BlockSpec((depth, width), lambda k: (k, 0)),
        ],
        out_specs=(whole(rows_dev, width),) * 2,
        scratch_shapes=[pltpu.VMEM((2 * rows_dev, width), f32)],
        name="project",
    )(core.astype(jnp.int32)[None], mine, projection)
    got = swap_cores(send)
    stream, outgoing = pl.pallas_call(
        dispatch_kernel,
        out_shape=(
            jax.ShapeDtypeStruct((rows_dev, width), bf16),
            jax.ShapeDtypeStruct((slot_count * PIECES, width // PIECES), bf16),
        ),
        in_specs=[VMEM] * 5,
        out_specs=(VMEM,) * 2,
        name="dispatch",
    )(keep, got, resid, expert_norm_gain[None, :], line)
    packed = (experts, CAP * PIECES, width // PIECES)
    arrived = lax.all_to_all(outgoing.reshape(packed), "sp", 0, 0, tiled=True)
    arrived = arrived.reshape(slot_count, width)

    rows = lax.all_gather(arrived, "tp", axis=0, axis_index_groups=groups, tiled=True)
    arrived, down_own, gate_own, up_own = lax.optimization_barrier(
        (arrived, down_own, gate_weight[0], up_weight[0])
    )
    gate = natural(gate_own, swap_cores(gate_own), core, 1)
    upward = natural(up_own, swap_cores(up_own), core, 1)
    down = natural(down_own[:, None], swap_cores(down_own)[:, None], core, 1)
    down = jnp.moveaxis(down.reshape(tp, CORES * hidden, -1), 0, 1).reshape(CORES * hidden, width)
    depth = CORES * hidden
    block = rows.shape[0] // 4
    summed = pl.pallas_call(
        expert_kernel,
        grid=(4,),
        out_shape=jax.ShapeDtypeStruct(rows.shape, bf16),
        in_specs=[
            pl.BlockSpec((block, width), lambda k: (k, 0)),
            whole(width, depth),
            whole(width, depth),
            whole(depth, width),
        ],
        out_specs=pl.BlockSpec((block, width), lambda k: (k, 0)),
        name="experts",
    )(rows, gate, upward, down)
    result = lax.psum_scatter(
        summed, "tp", scatter_dimension=0, axis_index_groups=groups, tiled=True
    )

    returned = lax.all_to_all(result.reshape(packed), "sp", 0, 0, tiled=True)
    return pl.pallas_call(
        combine_kernel,
        out_shape=jax.ShapeDtypeStruct((rows_dev, width), bf16),
        in_specs=[VMEM] * 4,
        out_specs=VMEM,
        name="combine",
    )(stream, returned.reshape(slot_count * PIECES, width // PIECES), column, expert_pair_weight)


def solution(mesh):
    placed = (
        P(("sp", "tp"), None),
        P("sp", "tp"),
        P("sp", "tp"),
        P(None, "tp"),
        P("tp", None, None),
        P("tp", None, None),
        P("tp"),
        P("sp", "tp"),
        P("tp", None),
        P(),
        P("sp", None),
        P(("sp", "tp"), None),
        P("sp", None, "tp"),
        P("sp", None, "tp"),
        P("sp", None, "tp"),
    )
    return jax.shard_map(
        layer, mesh=mesh, in_specs=placed, out_specs=P(("sp", "tp"), None), check_vma=False
    )
```

```python
import jax
import jax.numpy as jnp
from jax import lax
from jax.experimental import pallas as pl
from jax.experimental.pallas import tpu as pltpu
from jax.sharding import PartitionSpec as P


RECURRENT_SCALE = 8.0
EPSILON = 1e-06
SEGMENTS = 8
CORES = 2
CAP = 3
PIECES = 8
GELU_SCALE = 0.7978845608028654

VMEM = pl.BlockSpec(memory_space=pltpu.VMEM)
SMEM = pl.BlockSpec(memory_space=pltpu.SMEM)


def shifted(block, axis, distance):
    devices = range(lax.axis_size(axis))
    route = [(i - distance, i) for i in devices if i - distance in devices]
    return lax.ppermute(block, axis, route)


def core_groups(size):
    return [[core + CORES * y for y in range(size // CORES)] for core in range(CORES)]


def swap_cores(x):
    size = lax.axis_size("tp")
    return lax.ppermute(x, "tp", [(i, i ^ 1) for i in range(size)])


def minus_expm1(x):
    series = 1.0 + x * (1.0 / 7.0)
    for k in (6, 5, 4, 3, 2):
        series = 1.0 + x * (1.0 / k) * series
    return jnp.where(x > -0.35, -x * series, 1.0 - jnp.exp(x))


def recurrence_kernel(
    x_ref, rim_ref, filter_ref, recur_ref, input_ref, raw_ref, boost_ref,
    state_ref, running_ref, total_ref, ext, decay, drive, gates,
):
    tokens, channels = x_ref.shape
    taps = filter_ref.shape[0]
    blocks, wide, _ = recur_ref.shape
    gates[...] = jnp.zeros_like(gates)
    for at, matrix in ((0, recur_ref), (channels, input_ref)):
        for k in range(blocks):
            low = k * wide
            gates[low : low + wide, at + low : at + low + wide] = matrix[k]
    lead = 8
    ext[lead - taps + 1 : lead, :] = rim_ref[...].astype(jnp.float32)
    ext[lead : lead + tokens, :] = x_ref[...].astype(jnp.float32)
    first = lead - taps + 1
    mixed = ext[first : first + tokens, :] * filter_ref[0:1, :]
    for k in range(1, taps):
        mixed = mixed + ext[first + k : first + k + tokens, :] * filter_ref[k : k + 1, :]
    smoothed = mixed.astype(jnp.bfloat16)
    logits = jnp.dot(smoothed, gates[...], preferred_element_type=jnp.float32)
    both = jax.nn.sigmoid(logits)
    minus_raw = -raw_ref[...]
    soft = jnp.maximum(minus_raw, 0.0) + jnp.log1p(jnp.exp(-jnp.abs(minus_raw)))
    log_decay = both[:, :channels] * (-RECURRENT_SCALE * soft) + boost_ref[...]
    decay[...] = jnp.exp(log_decay)
    drive[...] = jnp.sqrt(minus_expm1(2.0 * log_decay)) * (
        both[:, channels:] * smoothed.astype(jnp.float32)
    )
    length = tokens // SEGMENTS

    def step(i, held):
        state, running = held
        rows = pl.ds(i, SEGMENTS, stride=length)
        a, b = decay[rows, :], drive[rows, :]
        state, running = a * state + b, running * a
        state_ref[rows, :] = state
        running_ref[rows, :] = running
        return state, running

    start = (jnp.zeros((SEGMENTS, channels), jnp.float32), jnp.ones((SEGMENTS, channels), jnp.float32))
    state, running = lax.fori_loop(0, length, step, start, unroll=8)
    whole_a, whole_b = running[0:1], state[0:1]
    for k in range(1, SEGMENTS):
        whole_b = running[k : k + 1] * whole_b + state[k : k + 1]
        whole_a = whole_a * running[k : k + 1]
    total_ref[:, 0:1, :] = jnp.broadcast_to(whole_a[None], (total_ref.shape[0], 1, channels))
    total_ref[:, 1:2, :] = jnp.broadcast_to(whole_b[None], (total_ref.shape[0], 1, channels))


def branch_kernel(place_ref, pieces_ref, state_ref, running_ref, gate_ref, keep_ref, send_ref):
    place, core = place_ref[0], place_ref[1]
    carry = jnp.zeros((1, state_ref.shape[1]), jnp.float32)
    for k in range(pieces_ref.shape[0]):
        after = pieces_ref[k, 0:1, :] * carry + pieces_ref[k, 1:2, :]
        carry = jnp.where(k < place, after, carry)
    length = state_ref.shape[0] // SEGMENTS
    half = length // CORES
    for k in range(SEGMENTS):
        for out, side in ((keep_ref, core), (send_ref, 1 - core)):
            rows = pl.ds(pl.multiple_of(k * length + side * half, half), half)
            state = state_ref[rows, :] + running_ref[rows, :] * carry
            g = gate_ref[rows, :].astype(jnp.float32)
            gelu = 0.5 * g * (1.0 + jnp.tanh(GELU_SCALE * (g + 0.044715 * (g * g * g))))
            out[k * half : (k + 1) * half, :] = (gelu * state).astype(jnp.bfloat16)
        last = (k + 1) * length - 1
        carry = running_ref[last : last + 1, :] * carry + state_ref[last : last + 1, :]


def slots_kernel(routes_ref, column_ref, line_ref):
    rows = routes_ref.shape[0]
    experts = 32
    number = lax.broadcasted_iota(jnp.int32, (rows, experts), 1)
    hot = [(routes_ref[:, k : k + 1] == number).astype(jnp.float32) for k in range(2)]
    earlier = (
        lax.broadcasted_iota(jnp.int32, (rows, rows), 1)
        < lax.broadcasted_iota(jnp.int32, (rows, rows), 0)
    ).astype(jnp.float32)
    before = jnp.dot(earlier, hot[0] + hot[1], preferred_element_type=jnp.float32)
    wide = line_ref.shape[1]
    lane = lax.broadcasted_iota(jnp.int32, (rows, wide), 1)
    same = lane % rows == lax.broadcasted_iota(jnp.int32, (rows, wide), 0)
    for k in range(2):
        rank = jnp.sum(before * hot[k], axis=1, keepdims=True).astype(jnp.int32)
        slot = routes_ref[:, k : k + 1] * CAP + rank
        column_ref[k * rows : (k + 1) * rows, :] = slot * PIECES
        spread = jnp.where(same, (slot * PIECES).astype(jnp.float32), 0.0)
        line_ref[k : k + 1, :] = (
            jnp.sum(spread, axis=0, keepdims=True).astype(jnp.int32) + lane[0:1] // rows
        )


def dispatch_kernel(parts_ref, resid_ref, gain_ref, line_ref, stream_ref, out_ref):
    rows, width = resid_ref.shape
    projected = parts_ref[0].astype(jnp.float32)
    for k in range(1, parts_ref.shape[0]):
        projected = projected + parts_ref[k].astype(jnp.float32)
    stream = (resid_ref[...].astype(jnp.float32) + projected).astype(jnp.bfloat16)
    stream_ref[...] = stream
    wide = stream.astype(jnp.float32)
    mean = jnp.sum(wide * wide, axis=1, keepdims=True) * (1.0 / width)
    normed = (wide * lax.rsqrt(mean + EPSILON) * gain_ref[...]).astype(jnp.bfloat16)
    piece = width // PIECES
    stacked = jnp.concatenate(
        [normed[:, k * piece : (k + 1) * piece] for k in range(PIECES)], axis=0
    )
    spot = lax.broadcasted_iota(jnp.int32, (out_ref.shape[0], rows * PIECES), 0)
    pick = (line_ref[0:1, :] == spot) | (line_ref[1:2, :] == spot)
    pick = pick.astype(jnp.float32).astype(jnp.bfloat16)
    out_ref[...] = jnp.dot(pick, stacked, preferred_element_type=jnp.float32).astype(jnp.bfloat16)


def expert_kernel(rows_ref, gate_ref, up_ref, down_ref, out_ref):
    rows = rows_ref[...]
    gate = jnp.dot(rows, gate_ref[...], preferred_element_type=jnp.float32)
    upward = jnp.dot(rows, up_ref[...], preferred_element_type=jnp.float32)
    active = (jax.nn.silu(gate) * upward).astype(jnp.bfloat16)
    out_ref[...] = jnp.dot(active, down_ref[...], preferred_element_type=jnp.float32).astype(
        jnp.bfloat16
    )


def combine_kernel(stream_ref, returned_ref, column_ref, weight_ref, out_ref):
    rows, width = stream_ref.shape
    piece = width // PIECES
    spot = lax.broadcasted_iota(jnp.int32, (2 * rows, returned_ref.shape[0]), 1)
    for k in range(PIECES):
        pick = (column_ref[...] + k == spot).astype(jnp.float32).astype(jnp.bfloat16)
        chosen = jnp.dot(pick, returned_ref[...], preferred_element_type=jnp.float32)
        lanes = slice(k * piece, (k + 1) * piece)
        total = weight_ref[:, 0:1] * chosen[:rows] + weight_ref[:, 1:2] * chosen[rows:]
        out_ref[:, lanes] = (stream_ref[:, lanes].astype(jnp.float32) + total).astype(jnp.bfloat16)


def natural(own, other, core, axis):
    return jnp.where(
        core == 0,
        jnp.concatenate([own, other], axis=axis),
        jnp.concatenate([other, own], axis=axis),
    )


def layer(
    resid,
    recurrent_input,
    recurrent_out_gate,
    filter_weight,
    recurrence_gate_matrix,
    input_gate_matrix,
    channel_decay_raw,
    token_decay_boost,
    output_projection_weight,
    expert_norm_gain,
    routes,
    expert_pair_weight,
    gate_weight,
    up_weight,
    down_weight,
):
    tokens, channels = recurrent_input.shape
    taps = filter_weight.shape[0]
    tp, experts = lax.axis_size("tp"), lax.axis_size("sp")
    here, place = lax.axis_index("tp"), lax.axis_index("sp")
    core = here % CORES
    chips = tp // CORES
    groups = core_groups(tp)
    rows_dev, width = resid.shape
    f32, bf16 = jnp.float32, jnp.bfloat16

    rim = shifted(recurrent_input[tokens - taps + 1 :], "sp", 1)
    projection_other = swap_cores(output_projection_weight)

    own_routes = lax.dynamic_slice_in_dim(routes, here * rows_dev, rows_dev, 0)
    column, line = pl.pallas_call(
        slots_kernel,
        out_shape=(
            jax.ShapeDtypeStruct((2 * rows_dev, 1), jnp.int32),
            jax.ShapeDtypeStruct((2, PIECES * rows_dev), jnp.int32),
        ),
        in_specs=[VMEM],
        out_specs=(VMEM,) * 2,
        name="slots",
    )(own_routes)

    state, running, total = pl.pallas_call(
        recurrence_kernel,
        out_shape=(
            jax.ShapeDtypeStruct((tokens, channels), f32),
            jax.ShapeDtypeStruct((tokens, channels), f32),
            jax.ShapeDtypeStruct((experts, 2, channels), f32),
        ),
        in_specs=[VMEM] * 7,
        out_specs=(VMEM,) * 3,
        scratch_shapes=[
            pltpu.VMEM((tokens + 8, channels), f32),
            pltpu.VMEM((tokens, channels), f32),
            pltpu.VMEM((tokens, channels), f32),
            pltpu.VMEM((channels, 2 * channels), bf16),
        ],
        cost_estimate=pl.CostEstimate(flops=10**9, bytes_accessed=2**20, transcendentals=0),
        name="recurrence",
    )(
        recurrent_input,
        rim,
        filter_weight,
        recurrence_gate_matrix,
        input_gate_matrix,
        channel_decay_raw[None, :],
        token_decay_boost,
    )

    pieces = lax.all_to_all(total, "sp", 0, 0, tiled=True)
    keep, send = pl.pallas_call(
        branch_kernel,
        out_shape=(jax.ShapeDtypeStruct((tokens // CORES, channels), bf16),) * 2,
        in_specs=[SMEM] + [VMEM] * 4,
        out_specs=(VMEM,) * 2,
        cost_estimate=pl.CostEstimate(flops=10**9, bytes_accessed=2**20, transcendentals=0),
        name="branch",
    )(jnp.stack([place, core]).astype(jnp.int32), pieces, state, running, recurrent_out_gate)
    got = swap_cores(send)
    both = jnp.concatenate([keep, got], axis=1)
    projection = jnp.concatenate([output_projection_weight, projection_other], axis=0)
    partial = jnp.dot(both, projection, preferred_element_type=f32).astype(bf16)
    parts = lax.all_to_all(
        partial.reshape(chips, rows_dev, width), "tp", 0, 0, axis_index_groups=groups, tiled=True
    )
    slot_count = experts * CAP
    whole = lambda *shape: pl.BlockSpec(shape, lambda k: (0,) * len(shape))
    stream, outgoing = pl.pallas_call(
        dispatch_kernel,
        out_shape=(
            jax.ShapeDtypeStruct((rows_dev, width), bf16),
            jax.ShapeDtypeStruct((slot_count * PIECES, width // PIECES), bf16),
        ),
        in_specs=[VMEM] * 4,
        out_specs=(VMEM,) * 2,
        name="dispatch",
    )(parts, resid, expert_norm_gain[None, :], line)
    packed = (experts, CAP * PIECES, width // PIECES)
    arrived = lax.all_to_all(outgoing.reshape(packed), "sp", 0, 0, tiled=True)
    arrived = arrived.reshape(slot_count, width)

    rows = lax.all_gather(arrived, "tp", axis=0, axis_index_groups=groups, tiled=True)
    arrived, down_part, gate_own, up_own = lax.optimization_barrier(
        (arrived, down_weight[0], gate_weight[0], up_weight[0])
    )
    hidden = gate_own.shape[1]
    down_own = lax.all_to_all(
        down_part.reshape(chips, CORES * hidden, -1), "tp", 0, 0,
        axis_index_groups=groups, tiled=True,
    )
    gate = natural(gate_own, swap_cores(gate_own), core, 1)
    upward = natural(up_own, swap_cores(up_own), core, 1)
    down = natural(down_own[:, None], swap_cores(down_own)[:, None], core, 1)
    down = jnp.moveaxis(down.reshape(tp, CORES * hidden, -1), 0, 1).reshape(CORES * hidden, width)
    depth = CORES * hidden
    block = rows.shape[0] // 4
    summed = pl.pallas_call(
        expert_kernel,
        grid=(4,),
        out_shape=jax.ShapeDtypeStruct(rows.shape, bf16),
        in_specs=[
            pl.BlockSpec((block, width), lambda k: (k, 0)),
            whole(width, depth),
            whole(width, depth),
            whole(depth, width),
        ],
        out_specs=pl.BlockSpec((block, width), lambda k: (k, 0)),
        name="experts",
    )(rows, gate, upward, down)
    result = lax.psum_scatter(
        summed, "tp", scatter_dimension=0, axis_index_groups=groups, tiled=True
    )

    returned = lax.all_to_all(result.reshape(packed), "sp", 0, 0, tiled=True)
    return pl.pallas_call(
        combine_kernel,
        out_shape=jax.ShapeDtypeStruct((rows_dev, width), bf16),
        in_specs=[VMEM] * 4,
        out_specs=VMEM,
        name="combine",
    )(stream, returned.reshape(slot_count * PIECES, width // PIECES), column, expert_pair_weight)


def solution(mesh):
    placed = (
        P(("sp", "tp"), None),
        P("sp", "tp"),
        P("sp", "tp"),
        P(None, "tp"),
        P("tp", None, None),
        P("tp", None, None),
        P("tp"),
        P("sp", "tp"),
        P("tp", None),
        P(),
        P("sp", None),
        P(("sp", "tp"), None),
        P("sp", None, "tp"),
        P("sp", None, "tp"),
        P("sp", None, "tp"),
    )
    return jax.shard_map(
        layer, mesh=mesh, in_specs=placed, out_specs=P(("sp", "tp"), None), check_vma=False
    )
```

```python
import jax
import jax.numpy as jnp
from jax import lax
from jax.experimental import pallas as pl
from jax.experimental.pallas import tpu as pltpu
from jax.sharding import PartitionSpec as P


RECURRENT_SCALE = 8.0
EPSILON = 1e-06
SEGMENTS = 8
CORES = 2
CAP = 3
QUAD = 4
EXPERT_STEPS = 2
PIECES = 8
GELU_SCALE = 0.7978845608028654

VMEM = pl.BlockSpec(memory_space=pltpu.VMEM)
SMEM = pl.BlockSpec(memory_space=pltpu.SMEM)


def shifted(block, axis, distance):
    devices = range(lax.axis_size(axis))
    route = [(i - distance, i) for i in devices if i - distance in devices]
    return lax.ppermute(block, axis, route)


def core_groups(size):
    return [[core + CORES * y for y in range(size // CORES)] for core in range(CORES)]


def swap_cores(x):
    size = lax.axis_size("tp")
    return lax.ppermute(x, "tp", [(i, i ^ 1) for i in range(size)])


def minus_expm1(x):
    series = 1.0 + x * (1.0 / 7.0)
    for k in (6, 5, 4, 3, 2):
        series = 1.0 + x * (1.0 / k) * series
    return jnp.where(x > -0.35, -x * series, 1.0 - jnp.exp(x))


def recurrence_kernel(
    x_ref, rim_ref, filter_ref, recur_ref, input_ref, raw_ref, boost_ref,
    state_ref, running_ref, total_ref, ext, decay, drive, gates,
):
    tokens, channels = x_ref.shape
    taps = filter_ref.shape[0]
    blocks, wide, _ = recur_ref.shape
    gates[...] = jnp.zeros_like(gates)
    for at, matrix in ((0, recur_ref), (channels, input_ref)):
        for k in range(blocks):
            low = k * wide
            gates[low : low + wide, at + low : at + low + wide] = matrix[k]
    lead = 8
    ext[lead - taps + 1 : lead, :] = rim_ref[...].astype(jnp.float32)
    ext[lead : lead + tokens, :] = x_ref[...].astype(jnp.float32)
    first = lead - taps + 1
    mixed = ext[first : first + tokens, :] * filter_ref[0:1, :]
    for k in range(1, taps):
        mixed = mixed + ext[first + k : first + k + tokens, :] * filter_ref[k : k + 1, :]
    smoothed = mixed.astype(jnp.bfloat16)
    logits = jnp.dot(smoothed, gates[...], preferred_element_type=jnp.float32)
    both = jax.nn.sigmoid(logits)
    minus_raw = -raw_ref[...]
    soft = jnp.maximum(minus_raw, 0.0) + jnp.log1p(jnp.exp(-jnp.abs(minus_raw)))
    log_decay = both[:, :channels] * (-RECURRENT_SCALE * soft) + boost_ref[...]
    decay[...] = jnp.exp(log_decay)
    drive[...] = jnp.sqrt(minus_expm1(2.0 * log_decay)) * (
        both[:, channels:] * smoothed.astype(jnp.float32)
    )
    length = tokens // SEGMENTS

    def step(i, held):
        state, running = held
        rows = pl.ds(i, SEGMENTS, stride=length)
        a, b = decay[rows, :], drive[rows, :]
        state, running = a * state + b, running * a
        state_ref[rows, :] = state
        running_ref[rows, :] = running
        return state, running

    start = (jnp.zeros((SEGMENTS, channels), jnp.float32), jnp.ones((SEGMENTS, channels), jnp.float32))
    state, running = lax.fori_loop(0, length, step, start, unroll=8)
    whole_a, whole_b = running[0:1], state[0:1]
    for k in range(1, SEGMENTS):
        whole_b = running[k : k + 1] * whole_b + state[k : k + 1]
        whole_a = whole_a * running[k : k + 1]
    total_ref[:, 0:1, :] = jnp.broadcast_to(whole_a[None], (total_ref.shape[0], 1, channels))
    total_ref[:, 1:2, :] = jnp.broadcast_to(whole_b[None], (total_ref.shape[0], 1, channels))


def branch_kernel(place_ref, pieces_ref, state_ref, running_ref, gate_ref, out_ref):
    place = place_ref[0]
    carry = jnp.zeros((1, state_ref.shape[1]), jnp.float32)
    for k in range(pieces_ref.shape[0]):
        after = pieces_ref[k, 0:1, :] * carry + pieces_ref[k, 1:2, :]
        carry = jnp.where(k < place, after, carry)
    length = state_ref.shape[0] // SEGMENTS
    half = length // CORES
    for k in range(SEGMENTS):
        rows = slice(k * length, (k + 1) * length)
        state = state_ref[rows, :] + running_ref[rows, :] * carry
        g = gate_ref[rows, :].astype(jnp.float32)
        gelu = 0.5 * g * (1.0 + jnp.tanh(GELU_SCALE * (g + 0.044715 * (g * g * g))))
        branch = (gelu * state).astype(jnp.bfloat16)
        for core in range(CORES):
            at = k * CORES + core
            low = at // QUAD * half
            out_ref[at % QUAD, low : low + half, :] = branch[core * half : (core + 1) * half]
        carry = state[length - 1 : length, :]


def project_kernel(branch_ref, weight_ref, out_ref):
    branch = jnp.concatenate([branch_ref[k] for k in range(branch_ref.shape[0])], axis=1)
    out_ref[...] = jnp.dot(branch, weight_ref[...], preferred_element_type=jnp.float32).astype(
        jnp.bfloat16
    )


def slots_kernel(routes_ref, column_ref, line_ref):
    rows = routes_ref.shape[0]
    experts = 32
    number = lax.broadcasted_iota(jnp.int32, (rows, experts), 1)
    hot = [(routes_ref[:, k : k + 1] == number).astype(jnp.float32) for k in range(2)]
    earlier = (
        lax.broadcasted_iota(jnp.int32, (rows, rows), 1)
        < lax.broadcasted_iota(jnp.int32, (rows, rows), 0)
    ).astype(jnp.float32)
    before = jnp.dot(earlier, hot[0] + hot[1], preferred_element_type=jnp.float32)
    wide = line_ref.shape[1]
    lane = lax.broadcasted_iota(jnp.int32, (rows, wide), 1)
    same = lane % rows == lax.broadcasted_iota(jnp.int32, (rows, wide), 0)
    for k in range(2):
        rank = jnp.sum(before * hot[k], axis=1, keepdims=True).astype(jnp.int32)
        slot = routes_ref[:, k : k + 1] * CAP + rank
        column_ref[k * rows : (k + 1) * rows, :] = slot * PIECES
        spread = jnp.where(same, (slot * PIECES).astype(jnp.float32), 0.0)
        line_ref[k : k + 1, :] = (
            jnp.sum(spread, axis=0, keepdims=True).astype(jnp.int32) + lane[0:1] // rows
        )


def dispatch_kernel(parts_ref, resid_ref, gain_ref, line_ref, stream_ref, out_ref):
    rows, width = resid_ref.shape
    projected = parts_ref[0].astype(jnp.float32)
    for k in range(1, parts_ref.shape[0]):
        projected = projected + parts_ref[k].astype(jnp.float32)
    stream = (resid_ref[...].astype(jnp.float32) + projected).astype(jnp.bfloat16)
    stream_ref[...] = stream
    wide = stream.astype(jnp.float32)
    mean = jnp.sum(wide * wide, axis=1, keepdims=True) * (1.0 / width)
    normed = (wide * lax.rsqrt(mean + EPSILON) * gain_ref[...]).astype(jnp.bfloat16)
    piece = width // PIECES
    stacked = jnp.concatenate(
        [normed[:, k * piece : (k + 1) * piece] for k in range(PIECES)], axis=0
    )
    spot = lax.broadcasted_iota(jnp.int32, (out_ref.shape[0], rows * PIECES), 0)
    pick = (line_ref[0:1, :] == spot) | (line_ref[1:2, :] == spot)
    pick = pick.astype(jnp.float32).astype(jnp.bfloat16)
    out_ref[...] = jnp.dot(pick, stacked, preferred_element_type=jnp.float32).astype(jnp.bfloat16)


def expert_kernel(rows_ref, gate_ref, up_ref, down_ref, out_ref):
    rows = rows_ref[...]
    gate = jnp.dot(rows, gate_ref[...], preferred_element_type=jnp.float32)
    upward = jnp.dot(rows, up_ref[...], preferred_element_type=jnp.float32)
    active = (jax.nn.silu(gate) * upward).astype(jnp.bfloat16)
    out_ref[...] = jnp.dot(active, down_ref[...], preferred_element_type=jnp.float32).astype(
        jnp.bfloat16
    )


def combine_kernel(stream_ref, returned_ref, column_ref, weight_ref, out_ref):
    rows, width = stream_ref.shape
    piece = width // PIECES
    spot = lax.broadcasted_iota(jnp.int32, (2 * rows, returned_ref.shape[0]), 1)
    for k in range(PIECES):
        pick = (column_ref[...] + k == spot).astype(jnp.float32).astype(jnp.bfloat16)
        chosen = jnp.dot(pick, returned_ref[...], preferred_element_type=jnp.float32)
        lanes = slice(k * piece, (k + 1) * piece)
        total = weight_ref[:, 0:1] * chosen[:rows] + weight_ref[:, 1:2] * chosen[rows:]
        out_ref[:, lanes] = (stream_ref[:, lanes].astype(jnp.float32) + total).astype(jnp.bfloat16)


def natural(own, other, core, axis):
    return jnp.where(
        core == 0,
        jnp.concatenate([own, other], axis=axis),
        jnp.concatenate([other, own], axis=axis),
    )


def layer(
    resid,
    recurrent_input,
    recurrent_out_gate,
    filter_weight,
    recurrence_gate_matrix,
    input_gate_matrix,
    channel_decay_raw,
    token_decay_boost,
    output_projection_weight,
    expert_norm_gain,
    routes,
    expert_pair_weight,
    gate_weight,
    up_weight,
    down_weight,
):
    tokens, channels = recurrent_input.shape
    taps = filter_weight.shape[0]
    tp, experts = lax.axis_size("tp"), lax.axis_size("sp")
    here, place = lax.axis_index("tp"), lax.axis_index("sp")
    core = here % CORES
    chips = tp // CORES
    groups = core_groups(tp)
    rows_dev, width = resid.shape
    f32, bf16 = jnp.float32, jnp.bfloat16

    rim = shifted(recurrent_input[tokens - taps + 1 :], "sp", 1)
    quads = [[k * QUAD + i for i in range(QUAD)] for k in range(tp // QUAD)]
    strides = [[k * QUAD + i for k in range(tp // QUAD)] for i in range(QUAD)]
    projection = lax.all_gather(
        output_projection_weight, "tp", axis=0, axis_index_groups=quads, tiled=True
    )

    own_routes = lax.dynamic_slice_in_dim(routes, here * rows_dev, rows_dev, 0)
    column, line = pl.pallas_call(
        slots_kernel,
        out_shape=(
            jax.ShapeDtypeStruct((2 * rows_dev, 1), jnp.int32),
            jax.ShapeDtypeStruct((2, PIECES * rows_dev), jnp.int32),
        ),
        in_specs=[VMEM],
        out_specs=(VMEM,) * 2,
        name="slots",
    )(own_routes)

    state, running, total = pl.pallas_call(
        recurrence_kernel,
        out_shape=(
            jax.ShapeDtypeStruct((tokens, channels), f32),
            jax.ShapeDtypeStruct((tokens, channels), f32),
            jax.ShapeDtypeStruct((experts, 2, channels), f32),
        ),
        in_specs=[VMEM] * 7,
        out_specs=(VMEM,) * 3,
        scratch_shapes=[
            pltpu.VMEM((tokens + 8, channels), f32),
            pltpu.VMEM((tokens, channels), f32),
            pltpu.VMEM((tokens, channels), f32),
            pltpu.VMEM((channels, 2 * channels), bf16),
        ],
        cost_estimate=pl.CostEstimate(flops=10**9, bytes_accessed=2**20, transcendentals=0),
        name="recurrence",
    )(
        recurrent_input,
        rim,
        filter_weight,
        recurrence_gate_matrix,
        input_gate_matrix,
        channel_decay_raw[None, :],
        token_decay_boost,
    )

    pieces = lax.all_to_all(total, "sp", 0, 0, tiled=True)
    branch = pl.pallas_call(
        branch_kernel,
        out_shape=jax.ShapeDtypeStruct((QUAD, tokens // QUAD, channels), bf16),
        in_specs=[SMEM] + [VMEM] * 4,
        out_specs=VMEM,
        name="branch",
    )(place.astype(jnp.int32)[None], pieces, state, running, recurrent_out_gate)
    mine = lax.all_to_all(branch, "tp", 0, 0, axis_index_groups=quads, tiled=True)
    cut = width // 2
    partial = pl.pallas_call(
        project_kernel,
        grid=(width // cut,),
        out_shape=jax.ShapeDtypeStruct((tokens // QUAD, width), bf16),
        in_specs=[
            pl.BlockSpec(mine.shape, lambda k: (0, 0, 0)),
            pl.BlockSpec((QUAD * channels, cut), lambda k: (0, k)),
        ],
        out_specs=pl.BlockSpec((tokens // QUAD, cut), lambda k: (0, k)),
        name="project",
    )(mine, projection)
    parts = lax.all_to_all(
        partial.reshape(tp // QUAD, rows_dev, width), "tp", 0, 0,
        axis_index_groups=strides, tiled=True,
    )
    slot_count = experts * CAP
    whole = lambda *shape: pl.BlockSpec(shape, lambda k: (0,) * len(shape))
    stream, outgoing = pl.pallas_call(
        dispatch_kernel,
        out_shape=(
            jax.ShapeDtypeStruct((rows_dev, width), bf16),
            jax.ShapeDtypeStruct((slot_count * PIECES, width // PIECES), bf16),
        ),
        in_specs=[VMEM] * 4,
        out_specs=(VMEM,) * 2,
        name="dispatch",
    )(parts, resid, expert_norm_gain[None, :], line)
    packed = (experts, CAP * PIECES, width // PIECES)
    arrived = lax.all_to_all(outgoing.reshape(packed), "sp", 0, 0, tiled=True)
    arrived = arrived.reshape(slot_count, width)

    rows = lax.all_gather(arrived, "tp", axis=0, axis_index_groups=groups, tiled=True)
    arrived, down_part, gate_own, up_own = lax.optimization_barrier(
        (arrived, down_weight[0], gate_weight[0], up_weight[0])
    )
    hidden = gate_own.shape[1]
    down_own = lax.all_to_all(
        down_part.reshape(chips, CORES * hidden, -1), "tp", 0, 0,
        axis_index_groups=groups, tiled=True,
    )
    gate = natural(gate_own, swap_cores(gate_own), core, 1)
    upward = natural(up_own, swap_cores(up_own), core, 1)
    down = natural(down_own[:, None], swap_cores(down_own)[:, None], core, 1)
    down = jnp.moveaxis(down.reshape(tp, CORES * hidden, -1), 0, 1).reshape(CORES * hidden, width)
    depth = CORES * hidden
    block = rows.shape[0] // EXPERT_STEPS
    summed = pl.pallas_call(
        expert_kernel,
        grid=(EXPERT_STEPS,),
        out_shape=jax.ShapeDtypeStruct(rows.shape, bf16),
        in_specs=[
            pl.BlockSpec((block, width), lambda k: (k, 0)),
            whole(width, depth),
            whole(width, depth),
            whole(depth, width),
        ],
        out_specs=pl.BlockSpec((block, width), lambda k: (k, 0)),
        name="experts",
    )(rows, gate, upward, down)
    result = lax.psum_scatter(
        summed, "tp", scatter_dimension=0, axis_index_groups=groups, tiled=True
    )

    returned = lax.all_to_all(result.reshape(packed), "sp", 0, 0, tiled=True)
    return pl.pallas_call(
        combine_kernel,
        out_shape=jax.ShapeDtypeStruct((rows_dev, width), bf16),
        in_specs=[VMEM] * 4,
        out_specs=VMEM,
        name="combine",
    )(stream, returned.reshape(slot_count * PIECES, width // PIECES), column, expert_pair_weight)


def solution(mesh):
    placed = (
        P(("sp", "tp"), None),
        P("sp", "tp"),
        P("sp", "tp"),
        P(None, "tp"),
        P("tp", None, None),
        P("tp", None, None),
        P("tp"),
        P("sp", "tp"),
        P("tp", None),
        P(),
        P("sp", None),
        P(("sp", "tp"), None),
        P("sp", None, "tp"),
        P("sp", None, "tp"),
        P("sp", None, "tp"),
    )
    return jax.shard_map(
        layer, mesh=mesh, in_specs=placed, out_specs=P(("sp", "tp"), None), check_vma=False
    )
```

```python
import jax
import jax.numpy as jnp
from jax import lax
from jax.experimental import pallas as pl
from jax.experimental.pallas import tpu as pltpu
from jax.sharding import PartitionSpec as P


RECURRENT_SCALE = 8.0
EPSILON = 1e-06
SEGMENTS = 8
CORES = 2
CAP = 3
QUAD = 4
EXPERT_STEPS = 2
PIECES = 8
GELU_SCALE = 0.7978845608028654

VMEM = pl.BlockSpec(memory_space=pltpu.VMEM)
SMEM = pl.BlockSpec(memory_space=pltpu.SMEM)


def shifted(block, axis, distance):
    devices = range(lax.axis_size(axis))
    route = [(i - distance, i) for i in devices if i - distance in devices]
    return lax.ppermute(block, axis, route)


def core_groups(size):
    return [[core + CORES * y for y in range(size // CORES)] for core in range(CORES)]


def swap_cores(x):
    size = lax.axis_size("tp")
    return lax.ppermute(x, "tp", [(i, i ^ 1) for i in range(size)])


def minus_expm1(x):
    series = 1.0 + x * (1.0 / 7.0)
    for k in (6, 5, 4, 3, 2):
        series = 1.0 + x * (1.0 / k) * series
    return jnp.where(x > -0.35, -x * series, 1.0 - jnp.exp(x))


def recurrence_kernel(
    x_ref, rim_ref, filter_ref, recur_ref, input_ref, raw_ref, boost_ref,
    state_ref, running_ref, total_ref, ext, decay, drive, gates,
):
    tokens, channels = x_ref.shape
    taps = filter_ref.shape[0]
    blocks, wide, _ = recur_ref.shape
    gates[...] = jnp.zeros_like(gates)
    for at, matrix in ((0, recur_ref), (channels, input_ref)):
        for k in range(blocks):
            low = k * wide
            gates[low : low + wide, at + low : at + low + wide] = matrix[k]
    lead = 8
    ext[lead - taps + 1 : lead, :] = rim_ref[...].astype(jnp.float32)
    ext[lead : lead + tokens, :] = x_ref[...].astype(jnp.float32)
    first = lead - taps + 1
    mixed = ext[first : first + tokens, :] * filter_ref[0:1, :]
    for k in range(1, taps):
        mixed = mixed + ext[first + k : first + k + tokens, :] * filter_ref[k : k + 1, :]
    smoothed = mixed.astype(jnp.bfloat16)
    logits = jnp.dot(smoothed, gates[...], preferred_element_type=jnp.float32)
    both = jax.nn.sigmoid(logits)
    minus_raw = -raw_ref[...]
    soft = jnp.maximum(minus_raw, 0.0) + jnp.log1p(jnp.exp(-jnp.abs(minus_raw)))
    log_decay = both[:, :channels] * (-RECURRENT_SCALE * soft) + boost_ref[...]
    decay[...] = jnp.exp(log_decay)
    drive[...] = jnp.sqrt(minus_expm1(2.0 * log_decay)) * (
        both[:, channels:] * smoothed.astype(jnp.float32)
    )
    length = tokens // SEGMENTS

    def step(i, held):
        state, running = held
        rows = pl.ds(i, SEGMENTS, stride=length)
        a, b = decay[rows, :], drive[rows, :]
        state, running = a * state + b, running * a
        state_ref[rows, :] = state
        running_ref[rows, :] = running
        return state, running

    start = (jnp.zeros((SEGMENTS, channels), jnp.float32), jnp.ones((SEGMENTS, channels), jnp.float32))
    state, running = lax.fori_loop(0, length, step, start, unroll=8)
    whole_a, whole_b = running[0:1], state[0:1]
    for k in range(1, SEGMENTS):
        whole_b = running[k : k + 1] * whole_b + state[k : k + 1]
        whole_a = whole_a * running[k : k + 1]
    total_ref[:, 0:1, :] = jnp.broadcast_to(whole_a[None], (total_ref.shape[0], 1, channels))
    total_ref[:, 1:2, :] = jnp.broadcast_to(whole_b[None], (total_ref.shape[0], 1, channels))


def branch_kernel(place_ref, pieces_ref, state_ref, running_ref, gate_ref, out_ref):
    place = place_ref[0]
    carry = jnp.zeros((1, state_ref.shape[1]), jnp.float32)
    for k in range(pieces_ref.shape[0]):
        after = pieces_ref[k, 0:1, :] * carry + pieces_ref[k, 1:2, :]
        carry = jnp.where(k < place, after, carry)
    length = state_ref.shape[0] // SEGMENTS
    half = length // CORES
    for k in range(SEGMENTS):
        rows = slice(k * length, (k + 1) * length)
        state = state_ref[rows, :] + running_ref[rows, :] * carry
        g = gate_ref[rows, :].astype(jnp.float32)
        gelu = 0.5 * g * (1.0 + jnp.tanh(GELU_SCALE * (g + 0.044715 * (g * g * g))))
        branch = (gelu * state).astype(jnp.bfloat16)
        for core in range(CORES):
            at = k * CORES + core
            low = at // QUAD * half
            out_ref[at % QUAD, low : low + half, :] = branch[core * half : (core + 1) * half]
        carry = state[length - 1 : length, :]


def project_kernel(branch_ref, weight_ref, out_ref):
    branch = jnp.concatenate([branch_ref[k] for k in range(branch_ref.shape[0])], axis=1)
    out_ref[...] = jnp.dot(branch, weight_ref[...], preferred_element_type=jnp.float32).astype(
        jnp.bfloat16
    )


def slots_kernel(routes_ref, weight_ref, column_ref, line_ref, pair_ref):
    pair_ref[...] = weight_ref[...]
    rows = routes_ref.shape[0]
    experts = 32
    number = lax.broadcasted_iota(jnp.int32, (rows, experts), 1)
    hot = [(routes_ref[:, k : k + 1] == number).astype(jnp.float32) for k in range(2)]
    earlier = (
        lax.broadcasted_iota(jnp.int32, (rows, rows), 1)
        < lax.broadcasted_iota(jnp.int32, (rows, rows), 0)
    ).astype(jnp.float32)
    before = jnp.dot(earlier, hot[0] + hot[1], preferred_element_type=jnp.float32)
    wide = line_ref.shape[1]
    lane = lax.broadcasted_iota(jnp.int32, (rows, wide), 1)
    same = lane % rows == lax.broadcasted_iota(jnp.int32, (rows, wide), 0)
    for k in range(2):
        rank = jnp.sum(before * hot[k], axis=1, keepdims=True).astype(jnp.int32)
        slot = routes_ref[:, k : k + 1] * CAP + rank
        column_ref[k * rows : (k + 1) * rows, :] = slot * PIECES
        spread = jnp.where(same, (slot * PIECES).astype(jnp.float32), 0.0)
        line_ref[k : k + 1, :] = (
            jnp.sum(spread, axis=0, keepdims=True).astype(jnp.int32) + lane[0:1] // rows
        )


def dispatch_kernel(parts_ref, resid_ref, gain_ref, line_ref, stream_ref, out_ref):
    rows, width = resid_ref.shape
    projected = parts_ref[0].astype(jnp.float32)
    for k in range(1, parts_ref.shape[0]):
        projected = projected + parts_ref[k].astype(jnp.float32)
    stream = (resid_ref[...].astype(jnp.float32) + projected).astype(jnp.bfloat16)
    stream_ref[...] = stream
    wide = stream.astype(jnp.float32)
    mean = jnp.sum(wide * wide, axis=1, keepdims=True) * (1.0 / width)
    normed = (wide * lax.rsqrt(mean + EPSILON) * gain_ref[...]).astype(jnp.bfloat16)
    piece = width // PIECES
    stacked = jnp.concatenate(
        [normed[:, k * piece : (k + 1) * piece] for k in range(PIECES)], axis=0
    )
    spot = lax.broadcasted_iota(jnp.int32, (out_ref.shape[0], rows * PIECES), 0)
    pick = (line_ref[0:1, :] == spot) | (line_ref[1:2, :] == spot)
    pick = pick.astype(jnp.float32).astype(jnp.bfloat16)
    out_ref[...] = jnp.dot(pick, stacked, preferred_element_type=jnp.float32).astype(jnp.bfloat16)


def expert_kernel(rows_ref, gate_ref, up_ref, down_ref, out_ref):
    rows = rows_ref[...]
    gate = jnp.dot(rows, gate_ref[...], preferred_element_type=jnp.float32)
    upward = jnp.dot(rows, up_ref[...], preferred_element_type=jnp.float32)
    active = (jax.nn.silu(gate) * upward).astype(jnp.bfloat16)
    out_ref[...] = jnp.dot(active, down_ref[...], preferred_element_type=jnp.float32).astype(
        jnp.bfloat16
    )


def combine_kernel(stream_ref, returned_ref, column_ref, weight_ref, out_ref):
    rows, width = stream_ref.shape
    piece = width // PIECES
    spot = lax.broadcasted_iota(jnp.int32, (2 * rows, returned_ref.shape[0]), 1)
    offset = spot - column_ref[...]
    pick = jnp.concatenate([(offset == k).astype(jnp.float32) for k in range(PIECES)], axis=0)
    chosen = jnp.dot(
        pick.astype(jnp.bfloat16), returned_ref[...], preferred_element_type=jnp.float32
    )
    for k in range(PIECES):
        lanes = slice(k * piece, (k + 1) * piece)
        low = 2 * rows * k
        total = (
            weight_ref[:, 0:1] * chosen[low : low + rows]
            + weight_ref[:, 1:2] * chosen[low + rows : low + 2 * rows]
        )
        out_ref[:, lanes] = (stream_ref[:, lanes].astype(jnp.float32) + total).astype(jnp.bfloat16)


def natural(own, other, core, axis):
    return jnp.where(
        core == 0,
        jnp.concatenate([own, other], axis=axis),
        jnp.concatenate([other, own], axis=axis),
    )


def layer(
    resid,
    recurrent_input,
    recurrent_out_gate,
    filter_weight,
    recurrence_gate_matrix,
    input_gate_matrix,
    channel_decay_raw,
    token_decay_boost,
    output_projection_weight,
    expert_norm_gain,
    routes,
    expert_pair_weight,
    gate_weight,
    up_weight,
    down_weight,
):
    tokens, channels = recurrent_input.shape
    taps = filter_weight.shape[0]
    tp, experts = lax.axis_size("tp"), lax.axis_size("sp")
    here, place = lax.axis_index("tp"), lax.axis_index("sp")
    core = here % CORES
    chips = tp // CORES
    groups = core_groups(tp)
    rows_dev, width = resid.shape
    f32, bf16 = jnp.float32, jnp.bfloat16

    rim = shifted(recurrent_input[tokens - taps + 1 :], "sp", 1)
    quads = [[k * QUAD + i for i in range(QUAD)] for k in range(tp // QUAD)]
    strides = [[k * QUAD + i for k in range(tp // QUAD)] for i in range(QUAD)]
    projection = lax.all_gather(
        output_projection_weight, "tp", axis=0, axis_index_groups=quads, tiled=True
    )

    state, running, total = pl.pallas_call(
        recurrence_kernel,
        out_shape=(
            jax.ShapeDtypeStruct((tokens, channels), f32),
            jax.ShapeDtypeStruct((tokens, channels), f32),
            jax.ShapeDtypeStruct((experts, 2, channels), f32),
        ),
        in_specs=[VMEM] * 7,
        out_specs=(VMEM,) * 3,
        scratch_shapes=[
            pltpu.VMEM((tokens + 8, channels), f32),
            pltpu.VMEM((tokens, channels), f32),
            pltpu.VMEM((tokens, channels), f32),
            pltpu.VMEM((channels, 2 * channels), bf16),
        ],
        cost_estimate=pl.CostEstimate(flops=10**9, bytes_accessed=2**20, transcendentals=0),
        name="recurrence",
    )(
        recurrent_input,
        rim,
        filter_weight,
        recurrence_gate_matrix,
        input_gate_matrix,
        channel_decay_raw[None, :],
        token_decay_boost,
    )

    pieces = lax.all_to_all(total, "sp", 0, 0, tiled=True)
    own_routes = lax.dynamic_slice_in_dim(routes, here * rows_dev, rows_dev, 0)
    own_routes, pair = lax.optimization_barrier((own_routes, expert_pair_weight, total))[:2]
    column, line, pair = pl.pallas_call(
        slots_kernel,
        out_shape=(
            jax.ShapeDtypeStruct((2 * rows_dev, 1), jnp.int32),
            jax.ShapeDtypeStruct((2, PIECES * rows_dev), jnp.int32),
            jax.ShapeDtypeStruct(pair.shape, f32),
        ),
        in_specs=[VMEM] * 2,
        out_specs=(VMEM,) * 3,
        name="slots",
    )(own_routes, pair)
    branch = pl.pallas_call(
        branch_kernel,
        out_shape=jax.ShapeDtypeStruct((QUAD, tokens // QUAD, channels), bf16),
        in_specs=[SMEM] + [VMEM] * 4,
        out_specs=VMEM,
        name="branch",
    )(place.astype(jnp.int32)[None], pieces, state, running, recurrent_out_gate)
    mine = lax.all_to_all(branch, "tp", 0, 0, axis_index_groups=quads, tiled=True)
    cut = width // 2
    partial = pl.pallas_call(
        project_kernel,
        grid=(width // cut,),
        out_shape=jax.ShapeDtypeStruct((tokens // QUAD, width), bf16),
        in_specs=[
            pl.BlockSpec(mine.shape, lambda k: (0, 0, 0)),
            pl.BlockSpec((QUAD * channels, cut), lambda k: (0, k)),
        ],
        out_specs=pl.BlockSpec((tokens // QUAD, cut), lambda k: (0, k)),
        name="project",
    )(mine, projection)
    parts = lax.all_to_all(
        partial.reshape(tp // QUAD, rows_dev, width), "tp", 0, 0,
        axis_index_groups=strides, tiled=True,
    )
    slot_count = experts * CAP
    whole = lambda *shape: pl.BlockSpec(shape, lambda k: (0,) * len(shape))
    stream, outgoing = pl.pallas_call(
        dispatch_kernel,
        out_shape=(
            jax.ShapeDtypeStruct((rows_dev, width), bf16),
            jax.ShapeDtypeStruct((slot_count * PIECES, width // PIECES), bf16),
        ),
        in_specs=[VMEM] * 4,
        out_specs=(VMEM,) * 2,
        name="dispatch",
    )(parts, resid, expert_norm_gain[None, :], line)
    packed = (experts, CAP * PIECES, width // PIECES)
    arrived = lax.all_to_all(outgoing.reshape(packed), "sp", 0, 0, tiled=True)
    arrived = arrived.reshape(slot_count, width)

    rows = lax.all_gather(arrived, "tp", axis=0, axis_index_groups=groups, tiled=True)
    arrived, down_part, gate_own, up_own = lax.optimization_barrier(
        (arrived, down_weight[0], gate_weight[0], up_weight[0])
    )
    hidden = gate_own.shape[1]
    down_own = lax.all_to_all(
        down_part.reshape(chips, CORES * hidden, -1), "tp", 0, 0,
        axis_index_groups=groups, tiled=True,
    )
    gate = natural(gate_own, swap_cores(gate_own), core, 1)
    upward = natural(up_own, swap_cores(up_own), core, 1)
    down = natural(down_own[:, None], swap_cores(down_own)[:, None], core, 1)
    down = jnp.moveaxis(down.reshape(tp, CORES * hidden, -1), 0, 1).reshape(CORES * hidden, width)
    depth = CORES * hidden
    block = rows.shape[0] // EXPERT_STEPS
    summed = pl.pallas_call(
        expert_kernel,
        grid=(EXPERT_STEPS,),
        out_shape=jax.ShapeDtypeStruct(rows.shape, bf16),
        in_specs=[
            pl.BlockSpec((block, width), lambda k: (k, 0)),
            whole(width, depth),
            whole(width, depth),
            whole(depth, width),
        ],
        out_specs=pl.BlockSpec((block, width), lambda k: (k, 0)),
        name="experts",
    )(rows, gate, upward, down)
    result = lax.psum_scatter(
        summed, "tp", scatter_dimension=0, axis_index_groups=groups, tiled=True
    )

    returned = lax.all_to_all(result.reshape(packed), "sp", 0, 0, tiled=True)
    return pl.pallas_call(
        combine_kernel,
        out_shape=jax.ShapeDtypeStruct((rows_dev, width), bf16),
        in_specs=[VMEM] * 4,
        out_specs=VMEM,
        name="combine",
    )(stream, returned.reshape(slot_count * PIECES, width // PIECES), column, pair)


def solution(mesh):
    placed = (
        P(("sp", "tp"), None),
        P("sp", "tp"),
        P("sp", "tp"),
        P(None, "tp"),
        P("tp", None, None),
        P("tp", None, None),
        P("tp"),
        P("sp", "tp"),
        P("tp", None),
        P(),
        P("sp", None),
        P(("sp", "tp"), None),
        P("sp", None, "tp"),
        P("sp", None, "tp"),
        P("sp", None, "tp"),
    )
    return jax.shard_map(
        layer, mesh=mesh, in_specs=placed, out_specs=P(("sp", "tp"), None), check_vma=False
    )
```

```python
import jax
import jax.numpy as jnp
from jax import lax
from jax.experimental import pallas as pl
from jax.experimental.pallas import tpu as pltpu
from jax.sharding import PartitionSpec as P


RECURRENT_SCALE = 8.0
EPSILON = 1e-06
SEGMENTS = 8
CORES = 2
CAP = 3
RIM = 16
QUAD = 4
EXPERT_STEPS = 2
PIECES = 8
GELU_SCALE = 0.7978845608028654

VMEM = pl.BlockSpec(memory_space=pltpu.VMEM)
SMEM = pl.BlockSpec(memory_space=pltpu.SMEM)


def shifted(block, axis, distance):
    devices = range(lax.axis_size(axis))
    route = [(i - distance, i) for i in devices if i - distance in devices]
    return lax.ppermute(block, axis, route)


def core_groups(size):
    return [[core + CORES * y for y in range(size // CORES)] for core in range(CORES)]


def swap_cores(x):
    size = lax.axis_size("tp")
    return lax.ppermute(x, "tp", [(i, i ^ 1) for i in range(size)])


def minus_expm1(x):
    series = 1.0 + x * (1.0 / 7.0)
    for k in (6, 5, 4, 3, 2):
        series = 1.0 + x * (1.0 / k) * series
    return jnp.where(x > -0.35, -x * series, 1.0 - jnp.exp(x))


def log_one_plus(x):
    series = 1.0 - x * (1.0 / 2.0 - x * (1.0 / 3.0 - x * (1.0 / 4.0 - x * (1.0 / 5.0))))
    return jnp.where(x < 0.02, x * series, jnp.log1p(x))


def recurrence_kernel(
    x_ref, rim_ref, filter_ref, recur_ref, input_ref, raw_ref, boost_ref,
    state_ref, running_ref, total_ref, ext, decay, drive, gates,
):
    tokens, channels = x_ref.shape
    taps = filter_ref.shape[0]
    blocks, wide, _ = recur_ref.shape
    gates[...] = jnp.zeros_like(gates)
    for at, matrix in ((0, recur_ref), (channels, input_ref)):
        for k in range(blocks):
            low = k * wide
            gates[low : low + wide, at + low : at + low + wide] = matrix[k]
    lead = 8
    ext[0:lead, :] = rim_ref[RIM - lead : RIM, :].astype(jnp.float32)
    ext[lead : lead + tokens, :] = x_ref[...].astype(jnp.float32)
    first = lead - taps + 1
    mixed = ext[first : first + tokens, :] * filter_ref[0:1, :]
    for k in range(1, taps):
        mixed = mixed + ext[first + k : first + k + tokens, :] * filter_ref[k : k + 1, :]
    smoothed = mixed.astype(jnp.bfloat16)
    logits = jnp.dot(smoothed, gates[...], preferred_element_type=jnp.float32)
    both = jax.nn.sigmoid(logits)
    minus_raw = -raw_ref[...]
    soft = jnp.maximum(minus_raw, 0.0) + log_one_plus(jnp.exp(-jnp.abs(minus_raw)))
    log_decay = both[:, :channels] * (-RECURRENT_SCALE * soft) + boost_ref[...]
    decay[...] = jnp.exp(log_decay)
    drive[...] = jnp.sqrt(minus_expm1(2.0 * log_decay)) * (
        both[:, channels:] * smoothed.astype(jnp.float32)
    )
    length = tokens // SEGMENTS

    def step(i, held):
        state, running = held
        rows = pl.ds(i, SEGMENTS, stride=length)
        a, b = decay[rows, :], drive[rows, :]
        state, running = a * state + b, running * a
        state_ref[rows, :] = state
        running_ref[rows, :] = running
        return state, running

    start = (jnp.zeros((SEGMENTS, channels), jnp.float32), jnp.ones((SEGMENTS, channels), jnp.float32))
    state, running = lax.fori_loop(0, length, step, start, unroll=8)
    whole_a, whole_b = running[0:1], state[0:1]
    for k in range(1, SEGMENTS):
        whole_b = running[k : k + 1] * whole_b + state[k : k + 1]
        whole_a = whole_a * running[k : k + 1]
    total_ref[:, 0:1, :] = jnp.broadcast_to(whole_a[None], (total_ref.shape[0], 1, channels))
    total_ref[:, 1:2, :] = jnp.broadcast_to(whole_b[None], (total_ref.shape[0], 1, channels))


def branch_kernel(place_ref, pieces_ref, state_ref, running_ref, gate_ref, out_ref):
    place = place_ref[0]
    carry = jnp.zeros((1, state_ref.shape[1]), jnp.float32)
    for k in range(pieces_ref.shape[0]):
        after = pieces_ref[k, 0:1, :] * carry + pieces_ref[k, 1:2, :]
        carry = jnp.where(k < place, after, carry)
    length = state_ref.shape[0] // SEGMENTS
    half = length // CORES
    for k in range(SEGMENTS):
        rows = slice(k * length, (k + 1) * length)
        state = state_ref[rows, :] + running_ref[rows, :] * carry
        g = gate_ref[rows, :].astype(jnp.float32)
        gelu = 0.5 * g * (1.0 + jnp.tanh(GELU_SCALE * (g + 0.044715 * (g * g * g))))
        branch = (gelu * state).astype(jnp.bfloat16)
        for core in range(CORES):
            at = k * CORES + core
            low = at // QUAD * half
            out_ref[at % QUAD, low : low + half, :] = branch[core * half : (core + 1) * half]
        carry = state[length - 1 : length, :]


def project_kernel(branch_ref, weight_ref, out_ref):
    branch = jnp.concatenate([branch_ref[k] for k in range(branch_ref.shape[0])], axis=1)
    out_ref[...] = jnp.dot(branch, weight_ref[...], preferred_element_type=jnp.float32).astype(
        jnp.bfloat16
    )


def slots_kernel(routes_ref, weight_ref, column_ref, line_ref, pair_ref):
    pair_ref[...] = weight_ref[...]
    rows = routes_ref.shape[0]
    experts = 32
    number = lax.broadcasted_iota(jnp.int32, (rows, experts), 1)
    hot = [(routes_ref[:, k : k + 1] == number).astype(jnp.float32) for k in range(2)]
    earlier = (
        lax.broadcasted_iota(jnp.int32, (rows, rows), 1)
        < lax.broadcasted_iota(jnp.int32, (rows, rows), 0)
    ).astype(jnp.float32)
    before = jnp.dot(earlier, hot[0] + hot[1], preferred_element_type=jnp.float32)
    wide = line_ref.shape[1]
    lane = lax.broadcasted_iota(jnp.int32, (rows, wide), 1)
    same = lane % rows == lax.broadcasted_iota(jnp.int32, (rows, wide), 0)
    for k in range(2):
        rank = jnp.sum(before * hot[k], axis=1, keepdims=True).astype(jnp.int32)
        slot = routes_ref[:, k : k + 1] * CAP + rank
        column_ref[k * rows : (k + 1) * rows, :] = slot * PIECES
        spread = jnp.where(same, (slot * PIECES).astype(jnp.float32), 0.0)
        line_ref[k : k + 1, :] = (
            jnp.sum(spread, axis=0, keepdims=True).astype(jnp.int32) + lane[0:1] // rows
        )


def dispatch_kernel(parts_ref, resid_ref, gain_ref, line_ref, stream_ref, out_ref):
    rows, width = resid_ref.shape
    projected = parts_ref[0].astype(jnp.float32)
    for k in range(1, parts_ref.shape[0]):
        projected = projected + parts_ref[k].astype(jnp.float32)
    stream = (resid_ref[...].astype(jnp.float32) + projected).astype(jnp.bfloat16)
    stream_ref[...] = stream
    wide = stream.astype(jnp.float32)
    mean = jnp.sum(wide * wide, axis=1, keepdims=True) * (1.0 / width)
    normed = (wide * lax.rsqrt(mean + EPSILON) * gain_ref[...]).astype(jnp.bfloat16)
    piece = width // PIECES
    stacked = jnp.concatenate(
        [normed[:, k * piece : (k + 1) * piece] for k in range(PIECES)], axis=0
    )
    spot = lax.broadcasted_iota(jnp.int32, (out_ref.shape[0], rows * PIECES), 0)
    pick = (line_ref[0:1, :] == spot) | (line_ref[1:2, :] == spot)
    pick = pick.astype(jnp.float32).astype(jnp.bfloat16)
    out_ref[...] = jnp.dot(pick, stacked, preferred_element_type=jnp.float32).astype(jnp.bfloat16)


def expert_kernel(rows_ref, gate_ref, up_ref, down_ref, out_ref):
    rows = rows_ref[...]
    gate = jnp.dot(rows, gate_ref[...], preferred_element_type=jnp.float32)
    upward = jnp.dot(rows, up_ref[...], preferred_element_type=jnp.float32)
    active = (jax.nn.silu(gate) * upward).astype(jnp.bfloat16)
    out_ref[...] = jnp.dot(active, down_ref[...], preferred_element_type=jnp.float32).astype(
        jnp.bfloat16
    )


def combine_kernel(stream_ref, returned_ref, column_ref, weight_ref, out_ref):
    rows, width = stream_ref.shape
    piece = width // PIECES
    spot = lax.broadcasted_iota(jnp.int32, (2 * rows, returned_ref.shape[0]), 1)
    offset = spot - column_ref[...]
    pick = jnp.concatenate([(offset == k).astype(jnp.float32) for k in range(PIECES)], axis=0)
    chosen = jnp.dot(
        pick.astype(jnp.bfloat16), returned_ref[...], preferred_element_type=jnp.float32
    )
    for k in range(PIECES):
        lanes = slice(k * piece, (k + 1) * piece)
        low = 2 * rows * k
        total = (
            weight_ref[:, 0:1] * chosen[low : low + rows]
            + weight_ref[:, 1:2] * chosen[low + rows : low + 2 * rows]
        )
        out_ref[:, lanes] = (stream_ref[:, lanes].astype(jnp.float32) + total).astype(jnp.bfloat16)


def natural(own, other, core, axis):
    return jnp.where(
        core == 0,
        jnp.concatenate([own, other], axis=axis),
        jnp.concatenate([other, own], axis=axis),
    )


def layer(
    resid,
    recurrent_input,
    recurrent_out_gate,
    filter_weight,
    recurrence_gate_matrix,
    input_gate_matrix,
    channel_decay_raw,
    token_decay_boost,
    output_projection_weight,
    expert_norm_gain,
    routes,
    expert_pair_weight,
    gate_weight,
    up_weight,
    down_weight,
):
    tokens, channels = recurrent_input.shape
    tp, experts = lax.axis_size("tp"), lax.axis_size("sp")
    here, place = lax.axis_index("tp"), lax.axis_index("sp")
    core = here % CORES
    chips = tp // CORES
    groups = core_groups(tp)
    rows_dev, width = resid.shape
    f32, bf16 = jnp.float32, jnp.bfloat16

    before = shifted(recurrent_input[tokens - RIM :], "sp", 1)
    quads = [[k * QUAD + i for i in range(QUAD)] for k in range(tp // QUAD)]
    strides = [[k * QUAD + i for k in range(tp // QUAD)] for i in range(QUAD)]
    projection = lax.all_gather(
        output_projection_weight, "tp", axis=0, axis_index_groups=quads, tiled=True
    )

    whole = lambda *shape: pl.BlockSpec(shape, lambda k: (0,) * len(shape))
    operands = (
        recurrent_input,
        before,
        filter_weight,
        recurrence_gate_matrix,
        input_gate_matrix,
        channel_decay_raw[None, :],
        token_decay_boost,
    )
    shapes = ((tokens, channels), (tokens, channels), (experts, 2, channels))
    state, running, total = pl.pallas_call(
        recurrence_kernel,
        out_shape=tuple(jax.ShapeDtypeStruct(shape, f32) for shape in shapes),
        in_specs=[VMEM] * len(operands),
        out_specs=(VMEM,) * len(shapes),
        scratch_shapes=[
            pltpu.VMEM((tokens + 8, channels), f32),
            pltpu.VMEM((tokens, channels), f32),
            pltpu.VMEM((tokens, channels), f32),
            pltpu.VMEM((channels, 2 * channels), bf16),
        ],
        cost_estimate=pl.CostEstimate(flops=10**9, bytes_accessed=2**20, transcendentals=0),
        name="recurrence",
    )(*operands)

    pieces = lax.all_to_all(total, "sp", 0, 0, tiled=True)
    own_routes = lax.dynamic_slice_in_dim(routes, here * rows_dev, rows_dev, 0)
    own_routes, pair = lax.optimization_barrier((own_routes, expert_pair_weight, total))[:2]
    column, line, pair = pl.pallas_call(
        slots_kernel,
        out_shape=(
            jax.ShapeDtypeStruct((2 * rows_dev, 1), jnp.int32),
            jax.ShapeDtypeStruct((2, PIECES * rows_dev), jnp.int32),
            jax.ShapeDtypeStruct(pair.shape, f32),
        ),
        in_specs=[VMEM] * 2,
        out_specs=(VMEM,) * 3,
        name="slots",
    )(own_routes, pair)
    branch = pl.pallas_call(
        branch_kernel,
        out_shape=jax.ShapeDtypeStruct((QUAD, tokens // QUAD, channels), bf16),
        in_specs=[SMEM] + [VMEM] * 4,
        out_specs=VMEM,
        name="branch",
    )(place.astype(jnp.int32)[None], pieces, state, running, recurrent_out_gate)
    mine = lax.all_to_all(branch, "tp", 0, 0, axis_index_groups=quads, tiled=True)
    cut = width // 2
    partial = pl.pallas_call(
        project_kernel,
        grid=(width // cut,),
        out_shape=jax.ShapeDtypeStruct((tokens // QUAD, width), bf16),
        in_specs=[
            pl.BlockSpec(mine.shape, lambda k: (0, 0, 0)),
            pl.BlockSpec((QUAD * channels, cut), lambda k: (0, k)),
        ],
        out_specs=pl.BlockSpec((tokens // QUAD, cut), lambda k: (0, k)),
        name="project",
    )(mine, projection)
    parts = lax.all_to_all(
        partial.reshape(tp // QUAD, rows_dev, width), "tp", 0, 0,
        axis_index_groups=strides, tiled=True,
    )
    slot_count = experts * CAP
    stream, outgoing = pl.pallas_call(
        dispatch_kernel,
        out_shape=(
            jax.ShapeDtypeStruct((rows_dev, width), bf16),
            jax.ShapeDtypeStruct((slot_count * PIECES, width // PIECES), bf16),
        ),
        in_specs=[VMEM] * 4,
        out_specs=(VMEM,) * 2,
        name="dispatch",
    )(parts, resid, expert_norm_gain[None, :], line)
    packed = (experts, CAP * PIECES, width // PIECES)
    arrived = lax.all_to_all(outgoing.reshape(packed), "sp", 0, 0, tiled=True)
    arrived = arrived.reshape(slot_count, width)

    rows = lax.all_gather(arrived, "tp", axis=0, axis_index_groups=groups, tiled=True)
    arrived, down_part, gate_own, up_own = lax.optimization_barrier(
        (arrived, down_weight[0], gate_weight[0], up_weight[0])
    )
    hidden = gate_own.shape[1]
    down_own = lax.all_to_all(
        down_part.reshape(chips, CORES * hidden, -1), "tp", 0, 0,
        axis_index_groups=groups, tiled=True,
    )
    gate = natural(gate_own, swap_cores(gate_own), core, 1)
    upward = natural(up_own, swap_cores(up_own), core, 1)
    down = natural(down_own[:, None], swap_cores(down_own)[:, None], core, 1)
    down = jnp.moveaxis(down.reshape(tp, CORES * hidden, -1), 0, 1).reshape(CORES * hidden, width)
    depth = CORES * hidden
    block = rows.shape[0] // EXPERT_STEPS
    summed = pl.pallas_call(
        expert_kernel,
        grid=(EXPERT_STEPS,),
        out_shape=jax.ShapeDtypeStruct(rows.shape, bf16),
        in_specs=[
            pl.BlockSpec((block, width), lambda k: (k, 0)),
            whole(width, depth),
            whole(width, depth),
            whole(depth, width),
        ],
        out_specs=pl.BlockSpec((block, width), lambda k: (k, 0)),
        name="experts",
    )(rows, gate, upward, down)
    result = lax.psum_scatter(
        summed, "tp", scatter_dimension=0, axis_index_groups=groups, tiled=True
    )

    returned = lax.all_to_all(result.reshape(packed), "sp", 0, 0, tiled=True)
    return pl.pallas_call(
        combine_kernel,
        out_shape=jax.ShapeDtypeStruct((rows_dev, width), bf16),
        in_specs=[VMEM] * 4,
        out_specs=VMEM,
        name="combine",
    )(stream, returned.reshape(slot_count * PIECES, width // PIECES), column, pair)


def solution(mesh):
    placed = (
        P(("sp", "tp"), None),
        P("sp", "tp"),
        P("sp", "tp"),
        P(None, "tp"),
        P("tp", None, None),
        P("tp", None, None),
        P("tp"),
        P("sp", "tp"),
        P("tp", None),
        P(),
        P("sp", None),
        P(("sp", "tp"), None),
        P("sp", None, "tp"),
        P("sp", None, "tp"),
        P("sp", None, "tp"),
    )
    return jax.shard_map(
        layer, mesh=mesh, in_specs=placed, out_specs=P(("sp", "tp"), None), check_vma=False
    )
```

```python
import jax
import jax.numpy as jnp
from jax import lax
from jax.experimental import pallas as pl
from jax.experimental.pallas import tpu as pltpu
from jax.sharding import PartitionSpec as P


RECURRENT_SCALE = 8.0
EPSILON = 1e-06
SEGMENTS = 8
CORES = 2
CAP = 3
RIM = 16
QUAD = 4
EXPERT_STEPS = 2
PIECES = 8
GELU_SCALE = 0.7978845608028654

VMEM = pl.BlockSpec(memory_space=pltpu.VMEM)
SMEM = pl.BlockSpec(memory_space=pltpu.SMEM)


def shifted(block, axis, distance):
    devices = range(lax.axis_size(axis))
    route = [(i - distance, i) for i in devices if i - distance in devices]
    return lax.ppermute(block, axis, route)


def core_groups(size):
    return [[core + CORES * y for y in range(size // CORES)] for core in range(CORES)]


def swap_cores(x):
    size = lax.axis_size("tp")
    return lax.ppermute(x, "tp", [(i, i ^ 1) for i in range(size)])


def minus_expm1(x):
    series = 1.0 + x * (1.0 / 7.0)
    for k in (6, 5, 4, 3, 2):
        series = 1.0 + x * (1.0 / k) * series
    return jnp.where(x > -0.35, -x * series, 1.0 - jnp.exp(x))


def log_one_plus(x):
    series = 1.0 - x * (1.0 / 2.0 - x * (1.0 / 3.0 - x * (1.0 / 4.0 - x * (1.0 / 5.0))))
    return jnp.where(x < 0.02, x * series, jnp.log1p(x))


def recurrence_kernel(
    x_ref, rim_ref, filter_ref, recur_ref, input_ref, raw_ref, boost_ref,
    state_ref, running_ref, total_ref, ext, decay, drive, gates,
):
    tokens, channels = x_ref.shape
    taps = filter_ref.shape[0]
    blocks, wide, _ = recur_ref.shape
    gates[...] = jnp.zeros_like(gates)
    for at, matrix in ((0, recur_ref), (channels, input_ref)):
        for k in range(blocks):
            low = k * wide
            gates[low : low + wide, at + low : at + low + wide] = matrix[k]
    lead = 8
    ext[0:lead, :] = rim_ref[RIM - lead : RIM, :].astype(jnp.float32)
    ext[lead : lead + tokens, :] = x_ref[...].astype(jnp.float32)
    first = lead - taps + 1
    mixed = ext[first : first + tokens, :] * filter_ref[0:1, :]
    for k in range(1, taps):
        mixed = mixed + ext[first + k : first + k + tokens, :] * filter_ref[k : k + 1, :]
    smoothed = mixed.astype(jnp.bfloat16)
    logits = jnp.dot(smoothed, gates[...], preferred_element_type=jnp.float32)
    both = jax.nn.sigmoid(logits)
    minus_raw = -raw_ref[...]
    soft = jnp.maximum(minus_raw, 0.0) + log_one_plus(jnp.exp(-jnp.abs(minus_raw)))
    log_decay = both[:, :channels] * (-RECURRENT_SCALE * soft) + boost_ref[...]
    decay[...] = jnp.exp(log_decay)
    drive[...] = jnp.sqrt(minus_expm1(2.0 * log_decay)) * (
        both[:, channels:] * smoothed.astype(jnp.float32)
    )
    length = tokens // SEGMENTS

    def step(i, held):
        state, running = held
        rows = pl.ds(i, SEGMENTS, stride=length)
        a, b = decay[rows, :], drive[rows, :]
        state, running = a * state + b, running * a
        state_ref[rows, :] = state
        running_ref[rows, :] = running
        return state, running

    start = (jnp.zeros((SEGMENTS, channels), jnp.float32), jnp.ones((SEGMENTS, channels), jnp.float32))
    state, running = lax.fori_loop(0, length, step, start, unroll=8)
    whole_a, whole_b = running[0:1], state[0:1]
    for k in range(1, SEGMENTS):
        whole_b = running[k : k + 1] * whole_b + state[k : k + 1]
        whole_a = whole_a * running[k : k + 1]
    total_ref[:, 0:1, :] = jnp.broadcast_to(whole_a[None], (total_ref.shape[0], 1, channels))
    total_ref[:, 1:2, :] = jnp.broadcast_to(whole_b[None], (total_ref.shape[0], 1, channels))


def branch_kernel(place_ref, pieces_ref, state_ref, running_ref, gate_ref, out_ref):
    place = place_ref[0]
    carry = jnp.zeros((1, state_ref.shape[1]), jnp.float32)
    for k in range(pieces_ref.shape[0]):
        after = pieces_ref[k, 0:1, :] * carry + pieces_ref[k, 1:2, :]
        carry = jnp.where(k < place, after, carry)
    length = state_ref.shape[0] // SEGMENTS
    half = length // CORES
    for k in range(SEGMENTS):
        rows = slice(k * length, (k + 1) * length)
        state = state_ref[rows, :] + running_ref[rows, :] * carry
        g = gate_ref[rows, :].astype(jnp.float32)
        gelu = 0.5 * g * (1.0 + jnp.tanh(GELU_SCALE * (g + 0.044715 * (g * g * g))))
        branch = (gelu * state).astype(jnp.bfloat16)
        for core in range(CORES):
            at = k * CORES + core
            low = at // QUAD * half
            out_ref[at % QUAD, low : low + half, :] = branch[core * half : (core + 1) * half]
        carry = state[length - 1 : length, :]


def project_kernel(branch_ref, weight_ref, out_ref):
    branch = jnp.concatenate([branch_ref[k] for k in range(branch_ref.shape[0])], axis=1)
    out_ref[...] = jnp.dot(branch, weight_ref[...], preferred_element_type=jnp.float32).astype(
        jnp.bfloat16
    )


def slots_kernel(routes_ref, weight_ref, column_ref, line_ref, pair_ref):
    pair_ref[...] = weight_ref[...]
    rows = routes_ref.shape[0]
    experts = 32
    number = lax.broadcasted_iota(jnp.int32, (rows, experts), 1)
    hot = [(routes_ref[:, k : k + 1] == number).astype(jnp.float32) for k in range(2)]
    earlier = (
        lax.broadcasted_iota(jnp.int32, (rows, rows), 1)
        < lax.broadcasted_iota(jnp.int32, (rows, rows), 0)
    ).astype(jnp.float32)
    before = jnp.dot(earlier, hot[0] + hot[1], preferred_element_type=jnp.float32)
    wide = line_ref.shape[1]
    lane = lax.broadcasted_iota(jnp.int32, (rows, wide), 1)
    same = lane % rows == lax.broadcasted_iota(jnp.int32, (rows, wide), 0)
    for k in range(2):
        rank = jnp.sum(before * hot[k], axis=1, keepdims=True).astype(jnp.int32)
        slot = routes_ref[:, k : k + 1] * CAP + rank
        column_ref[k * rows : (k + 1) * rows, :] = slot * PIECES
        spread = jnp.where(same, (slot * PIECES).astype(jnp.float32), 0.0)
        line_ref[k : k + 1, :] = (
            jnp.sum(spread, axis=0, keepdims=True).astype(jnp.int32) + lane[0:1] // rows
        )


def dispatch_kernel(parts_ref, resid_ref, gain_ref, line_ref, stream_ref, out_ref):
    rows, width = resid_ref.shape
    projected = parts_ref[0].astype(jnp.float32)
    for k in range(1, parts_ref.shape[0]):
        projected = projected + parts_ref[k].astype(jnp.float32)
    stream = (resid_ref[...].astype(jnp.float32) + projected).astype(jnp.bfloat16)
    stream_ref[...] = stream
    wide = stream.astype(jnp.float32)
    mean = jnp.sum(wide * wide, axis=1, keepdims=True) * (1.0 / width)
    normed = (wide * lax.rsqrt(mean + EPSILON) * gain_ref[...]).astype(jnp.bfloat16)
    piece = width // PIECES
    stacked = jnp.concatenate(
        [normed[:, k * piece : (k + 1) * piece] for k in range(PIECES)], axis=0
    )
    spot = lax.broadcasted_iota(jnp.int32, (out_ref.shape[0], rows * PIECES), 0)
    pick = (line_ref[0:1, :] == spot) | (line_ref[1:2, :] == spot)
    pick = pick.astype(jnp.float32).astype(jnp.bfloat16)
    out_ref[...] = jnp.dot(pick, stacked, preferred_element_type=jnp.float32).astype(jnp.bfloat16)


def expert_kernel(rows_ref, gate_ref, up_ref, down_ref, out_ref):
    rows = rows_ref[...]
    gate = jnp.dot(rows, gate_ref[...], preferred_element_type=jnp.float32)
    upward = jnp.dot(rows, up_ref[...], preferred_element_type=jnp.float32)
    active = (jax.nn.silu(gate) * upward).astype(jnp.bfloat16)
    out_ref[...] = jnp.dot(active, down_ref[...], preferred_element_type=jnp.float32).astype(
        jnp.bfloat16
    )


def combine_kernel(stream_ref, returned_ref, column_ref, weight_ref, out_ref):
    rows, width = stream_ref.shape
    piece = width // PIECES
    spot = lax.broadcasted_iota(jnp.int32, (2 * rows, returned_ref.shape[0]), 1)
    offset = spot - column_ref[...]
    pick = jnp.concatenate([(offset == k).astype(jnp.float32) for k in range(PIECES)], axis=0)
    chosen = jnp.dot(
        pick.astype(jnp.bfloat16), returned_ref[...], preferred_element_type=jnp.float32
    )
    for k in range(PIECES):
        lanes = slice(k * piece, (k + 1) * piece)
        low = 2 * rows * k
        total = (
            weight_ref[:, 0:1] * chosen[low : low + rows]
            + weight_ref[:, 1:2] * chosen[low + rows : low + 2 * rows]
        )
        out_ref[:, lanes] = (stream_ref[:, lanes].astype(jnp.float32) + total).astype(jnp.bfloat16)


def natural(own, other, core, axis):
    return jnp.where(
        core == 0,
        jnp.concatenate([own, other], axis=axis),
        jnp.concatenate([other, own], axis=axis),
    )


def layer(
    resid,
    recurrent_input,
    recurrent_out_gate,
    filter_weight,
    recurrence_gate_matrix,
    input_gate_matrix,
    channel_decay_raw,
    token_decay_boost,
    output_projection_weight,
    expert_norm_gain,
    routes,
    expert_pair_weight,
    gate_weight,
    up_weight,
    down_weight,
):
    tokens, channels = recurrent_input.shape
    tp, experts = lax.axis_size("tp"), lax.axis_size("sp")
    here, place = lax.axis_index("tp"), lax.axis_index("sp")
    core = here % CORES
    groups = core_groups(tp)
    rows_dev, width = resid.shape
    f32, bf16 = jnp.float32, jnp.bfloat16

    before = shifted(recurrent_input[tokens - RIM :], "sp", 1)
    quads = [[k * QUAD + i for i in range(QUAD)] for k in range(tp // QUAD)]
    strides = [[k * QUAD + i for k in range(tp // QUAD)] for i in range(QUAD)]
    projection = lax.all_gather(
        output_projection_weight, "tp", axis=0, axis_index_groups=quads, tiled=True
    )

    whole = lambda *shape: pl.BlockSpec(shape, lambda k: (0,) * len(shape))
    operands = (
        recurrent_input,
        before,
        filter_weight,
        recurrence_gate_matrix,
        input_gate_matrix,
        channel_decay_raw[None, :],
        token_decay_boost,
    )
    shapes = ((tokens, channels), (tokens, channels), (experts, 2, channels))
    state, running, total = pl.pallas_call(
        recurrence_kernel,
        out_shape=tuple(jax.ShapeDtypeStruct(shape, f32) for shape in shapes),
        in_specs=[VMEM] * len(operands),
        out_specs=(VMEM,) * len(shapes),
        scratch_shapes=[
            pltpu.VMEM((tokens + 8, channels), f32),
            pltpu.VMEM((tokens, channels), f32),
            pltpu.VMEM((tokens, channels), f32),
            pltpu.VMEM((channels, 2 * channels), bf16),
        ],
        cost_estimate=pl.CostEstimate(flops=10**9, bytes_accessed=2**20, transcendentals=0),
        name="recurrence",
    )(*operands)

    pieces = lax.all_to_all(total, "sp", 0, 0, tiled=True)
    down_all = lax.all_gather(down_weight[0], "tp", axis_index_groups=groups)
    own_routes = lax.dynamic_slice_in_dim(routes, here * rows_dev, rows_dev, 0)
    own_routes, pair = lax.optimization_barrier((own_routes, expert_pair_weight, total))[:2]
    column, line, pair = pl.pallas_call(
        slots_kernel,
        out_shape=(
            jax.ShapeDtypeStruct((2 * rows_dev, 1), jnp.int32),
            jax.ShapeDtypeStruct((2, PIECES * rows_dev), jnp.int32),
            jax.ShapeDtypeStruct(pair.shape, f32),
        ),
        in_specs=[VMEM] * 2,
        out_specs=(VMEM,) * 3,
        name="slots",
    )(own_routes, pair)
    branch = pl.pallas_call(
        branch_kernel,
        out_shape=jax.ShapeDtypeStruct((QUAD, tokens // QUAD, channels), bf16),
        in_specs=[SMEM] + [VMEM] * 4,
        out_specs=VMEM,
        name="branch",
    )(place.astype(jnp.int32)[None], pieces, state, running, recurrent_out_gate)
    mine = lax.all_to_all(branch, "tp", 0, 0, axis_index_groups=quads, tiled=True)
    cut = width // 2
    partial = pl.pallas_call(
        project_kernel,
        grid=(width // cut,),
        out_shape=jax.ShapeDtypeStruct((tokens // QUAD, width), bf16),
        in_specs=[
            pl.BlockSpec(mine.shape, lambda k: (0, 0, 0)),
            pl.BlockSpec((QUAD * channels, cut), lambda k: (0, k)),
        ],
        out_specs=pl.BlockSpec((tokens // QUAD, cut), lambda k: (0, k)),
        name="project",
    )(mine, projection)
    parts = lax.all_to_all(
        partial.reshape(tp // QUAD, rows_dev, width), "tp", 0, 0,
        axis_index_groups=strides, tiled=True,
    )
    slot_count = experts * CAP
    stream, outgoing = pl.pallas_call(
        dispatch_kernel,
        out_shape=(
            jax.ShapeDtypeStruct((rows_dev, width), bf16),
            jax.ShapeDtypeStruct((slot_count * PIECES, width // PIECES), bf16),
        ),
        in_specs=[VMEM] * 4,
        out_specs=(VMEM,) * 2,
        name="dispatch",
    )(parts, resid, expert_norm_gain[None, :], line)
    packed = (experts, CAP * PIECES, width // PIECES)
    arrived = lax.all_to_all(outgoing.reshape(packed), "sp", 0, 0, tiled=True)
    arrived = arrived.reshape(slot_count, width)

    rows = lax.all_gather(arrived, "tp", axis=0, axis_index_groups=groups, tiled=True)
    arrived, down_all, gate_own, up_own = lax.optimization_barrier(
        (arrived, down_all, gate_weight[0], up_weight[0])
    )
    hidden = gate_own.shape[1]
    down_own = lax.dynamic_slice_in_dim(
        down_all, here // CORES * CORES * hidden, CORES * hidden, 1
    )
    gate = natural(gate_own, swap_cores(gate_own), core, 1)
    upward = natural(up_own, swap_cores(up_own), core, 1)
    down = natural(down_own[:, None], swap_cores(down_own)[:, None], core, 1)
    down = jnp.moveaxis(down.reshape(tp, CORES * hidden, -1), 0, 1).reshape(CORES * hidden, width)
    depth = CORES * hidden
    block = rows.shape[0] // EXPERT_STEPS
    summed = pl.pallas_call(
        expert_kernel,
        grid=(EXPERT_STEPS,),
        out_shape=jax.ShapeDtypeStruct(rows.shape, bf16),
        in_specs=[
            pl.BlockSpec((block, width), lambda k: (k, 0)),
            whole(width, depth),
            whole(width, depth),
            whole(depth, width),
        ],
        out_specs=pl.BlockSpec((block, width), lambda k: (k, 0)),
        name="experts",
    )(rows, gate, upward, down)
    result = lax.psum_scatter(
        summed, "tp", scatter_dimension=0, axis_index_groups=groups, tiled=True
    )

    returned = lax.all_to_all(result.reshape(packed), "sp", 0, 0, tiled=True)
    return pl.pallas_call(
        combine_kernel,
        out_shape=jax.ShapeDtypeStruct((rows_dev, width), bf16),
        in_specs=[VMEM] * 4,
        out_specs=VMEM,
        name="combine",
    )(stream, returned.reshape(slot_count * PIECES, width // PIECES), column, pair)


def solution(mesh):
    placed = (
        P(("sp", "tp"), None),
        P("sp", "tp"),
        P("sp", "tp"),
        P(None, "tp"),
        P("tp", None, None),
        P("tp", None, None),
        P("tp"),
        P("sp", "tp"),
        P("tp", None),
        P(),
        P("sp", None),
        P(("sp", "tp"), None),
        P("sp", None, "tp"),
        P("sp", None, "tp"),
        P("sp", None, "tp"),
    )
    return jax.shard_map(
        layer, mesh=mesh, in_specs=placed, out_specs=P(("sp", "tp"), None), check_vma=False
    )
```

```python
import jax
import jax.numpy as jnp
from jax import lax
from jax.experimental import pallas as pl
from jax.experimental.pallas import tpu as pltpu
from jax.sharding import PartitionSpec as P


RECURRENT_SCALE = 8.0
EPSILON = 1e-06
SEGMENTS = 8
CORES = 2
CAP = 3
RIM = 16
QUAD = 4
EXPERT_STEPS = 2
PIECES = 8
GELU_SCALE = 0.7978845608028654

VMEM = pl.BlockSpec(memory_space=pltpu.VMEM)
SMEM = pl.BlockSpec(memory_space=pltpu.SMEM)


def shifted(block, axis, distance):
    devices = range(lax.axis_size(axis))
    route = [(i - distance, i) for i in devices if i - distance in devices]
    return lax.ppermute(block, axis, route)


def core_groups(size):
    return [[core + CORES * y for y in range(size // CORES)] for core in range(CORES)]


def swap_cores(x):
    size = lax.axis_size("tp")
    return lax.ppermute(x, "tp", [(i, i ^ 1) for i in range(size)])


def minus_expm1(x):
    series = 1.0 + x * (1.0 / 7.0)
    for k in (6, 5, 4, 3, 2):
        series = 1.0 + x * (1.0 / k) * series
    return jnp.where(x > -0.35, -x * series, 1.0 - jnp.exp(x))


def log_one_plus(x):
    series = 1.0 - x * (1.0 / 2.0 - x * (1.0 / 3.0 - x * (1.0 / 4.0 - x * (1.0 / 5.0))))
    return jnp.where(x < 0.02, x * series, jnp.log1p(x))


def recurrence_kernel(
    x_ref, rim_ref, filter_ref, recur_ref, input_ref, raw_ref, boost_ref,
    state_ref, running_ref, total_ref, ext, decay, drive, gates,
):
    tokens, channels = x_ref.shape
    taps = filter_ref.shape[0]
    blocks, wide, _ = recur_ref.shape
    gates[...] = jnp.zeros_like(gates)
    for at, matrix in ((0, recur_ref), (channels, input_ref)):
        for k in range(blocks):
            low = k * wide
            gates[low : low + wide, at + low : at + low + wide] = matrix[k]
    lead = 8
    ext[0:lead, :] = rim_ref[RIM - lead : RIM, :].astype(jnp.float32)
    ext[lead : lead + tokens, :] = x_ref[...].astype(jnp.float32)
    first = lead - taps + 1
    mixed = ext[first : first + tokens, :] * filter_ref[0:1, :]
    for k in range(1, taps):
        mixed = mixed + ext[first + k : first + k + tokens, :] * filter_ref[k : k + 1, :]
    smoothed = mixed.astype(jnp.bfloat16)
    logits = jnp.dot(smoothed, gates[...], preferred_element_type=jnp.float32)
    both = jax.nn.sigmoid(logits)
    minus_raw = -raw_ref[...]
    soft = jnp.maximum(minus_raw, 0.0) + log_one_plus(jnp.exp(-jnp.abs(minus_raw)))
    log_decay = both[:, :channels] * (-RECURRENT_SCALE * soft) + boost_ref[...]
    decay[...] = jnp.exp(log_decay)
    drive[...] = jnp.sqrt(minus_expm1(2.0 * log_decay)) * (
        both[:, channels:] * smoothed.astype(jnp.float32)
    )
    length = tokens // SEGMENTS

    def step(i, held):
        state, running = held
        rows = pl.ds(i, SEGMENTS, stride=length)
        a, b = decay[rows, :], drive[rows, :]
        state, running = a * state + b, running * a
        state_ref[rows, :] = state
        running_ref[rows, :] = running
        return state, running

    start = (jnp.zeros((SEGMENTS, channels), jnp.float32), jnp.ones((SEGMENTS, channels), jnp.float32))
    state, running = lax.fori_loop(0, length, step, start, unroll=8)
    whole_a, whole_b = running[0:1], state[0:1]
    for k in range(1, SEGMENTS):
        whole_b = running[k : k + 1] * whole_b + state[k : k + 1]
        whole_a = whole_a * running[k : k + 1]
    total_ref[:, 0:1, :] = jnp.broadcast_to(whole_a[None], (total_ref.shape[0], 1, channels))
    total_ref[:, 1:2, :] = jnp.broadcast_to(whole_b[None], (total_ref.shape[0], 1, channels))


def branch_kernel(place_ref, pieces_ref, state_ref, running_ref, gate_ref, out_ref):
    place = place_ref[0]
    carry = jnp.zeros((1, state_ref.shape[1]), jnp.float32)
    for k in range(pieces_ref.shape[0]):
        after = pieces_ref[k, 0:1, :] * carry + pieces_ref[k, 1:2, :]
        carry = jnp.where(k < place, after, carry)
    length = state_ref.shape[0] // SEGMENTS
    half = length // CORES
    for k in range(SEGMENTS):
        rows = slice(k * length, (k + 1) * length)
        state = state_ref[rows, :] + running_ref[rows, :] * carry
        g = gate_ref[rows, :].astype(jnp.float32)
        gelu = 0.5 * g * (1.0 + jnp.tanh(GELU_SCALE * (g + 0.044715 * (g * g * g))))
        branch = (gelu * state).astype(jnp.bfloat16)
        for core in range(CORES):
            at = k * CORES + core
            low = at // QUAD * half
            out_ref[at % QUAD, low : low + half, :] = branch[core * half : (core + 1) * half]
        carry = state[length - 1 : length, :]


def project_kernel(branch_ref, weight_ref, out_ref):
    branch = jnp.concatenate([branch_ref[k] for k in range(branch_ref.shape[0])], axis=1)
    out_ref[...] = jnp.dot(branch, weight_ref[...], preferred_element_type=jnp.float32).astype(
        jnp.bfloat16
    )


def slots_kernel(routes_ref, weight_ref, column_ref, line_ref, pair_ref):
    pair_ref[...] = weight_ref[...]
    rows = routes_ref.shape[0]
    experts = 32
    number = lax.broadcasted_iota(jnp.int32, (rows, experts), 1)
    hot = [(routes_ref[:, k : k + 1] == number).astype(jnp.float32) for k in range(2)]
    earlier = (
        lax.broadcasted_iota(jnp.int32, (rows, rows), 1)
        < lax.broadcasted_iota(jnp.int32, (rows, rows), 0)
    ).astype(jnp.float32)
    before = jnp.dot(earlier, hot[0] + hot[1], preferred_element_type=jnp.float32)
    wide = line_ref.shape[1]
    lane = lax.broadcasted_iota(jnp.int32, (rows, wide), 1)
    same = lane % rows == lax.broadcasted_iota(jnp.int32, (rows, wide), 0)
    for k in range(2):
        rank = jnp.sum(before * hot[k], axis=1, keepdims=True).astype(jnp.int32)
        slot = routes_ref[:, k : k + 1] * CAP + rank
        column_ref[k * rows : (k + 1) * rows, :] = slot * PIECES
        spread = jnp.where(same, (slot * PIECES).astype(jnp.float32), 0.0)
        line_ref[k : k + 1, :] = (
            jnp.sum(spread, axis=0, keepdims=True).astype(jnp.int32) + lane[0:1] // rows
        )


def dispatch_kernel(parts_ref, resid_ref, gain_ref, line_ref, stream_ref, out_ref):
    rows, width = resid_ref.shape
    projected = parts_ref[0].astype(jnp.float32)
    for k in range(1, parts_ref.shape[0]):
        projected = projected + parts_ref[k].astype(jnp.float32)
    stream = (resid_ref[...].astype(jnp.float32) + projected).astype(jnp.bfloat16)
    stream_ref[...] = stream
    wide = stream.astype(jnp.float32)
    mean = jnp.sum(wide * wide, axis=1, keepdims=True) * (1.0 / width)
    normed = (wide * lax.rsqrt(mean + EPSILON) * gain_ref[...]).astype(jnp.bfloat16)
    piece = width // PIECES
    stacked = jnp.concatenate(
        [normed[:, k * piece : (k + 1) * piece] for k in range(PIECES)], axis=0
    )
    spot = lax.broadcasted_iota(jnp.int32, (out_ref.shape[0], rows * PIECES), 0)
    pick = (line_ref[0:1, :] == spot) | (line_ref[1:2, :] == spot)
    pick = pick.astype(jnp.float32).astype(jnp.bfloat16)
    out_ref[...] = jnp.dot(pick, stacked, preferred_element_type=jnp.float32).astype(jnp.bfloat16)


def expert_kernel(rows_ref, gate_ref, up_ref, down_ref, out_ref):
    rows = rows_ref[...]
    gate = jnp.dot(rows, gate_ref[...], preferred_element_type=jnp.float32)
    upward = jnp.dot(rows, up_ref[...], preferred_element_type=jnp.float32)
    active = (jax.nn.silu(gate) * upward).astype(jnp.bfloat16)
    out_ref[...] = jnp.dot(active, down_ref[...], preferred_element_type=jnp.float32).astype(
        jnp.bfloat16
    )


def combine_kernel(stream_ref, returned_ref, column_ref, weight_ref, out_ref):
    rows, width = stream_ref.shape
    piece = width // PIECES
    spot = lax.broadcasted_iota(jnp.int32, (2 * rows, returned_ref.shape[0]), 1)
    offset = spot - column_ref[...]
    pick = jnp.concatenate([(offset == k).astype(jnp.float32) for k in range(PIECES)], axis=0)
    chosen = jnp.dot(
        pick.astype(jnp.bfloat16), returned_ref[...], preferred_element_type=jnp.float32
    )
    for k in range(PIECES):
        lanes = slice(k * piece, (k + 1) * piece)
        low = 2 * rows * k
        total = (
            weight_ref[:, 0:1] * chosen[low : low + rows]
            + weight_ref[:, 1:2] * chosen[low + rows : low + 2 * rows]
        )
        out_ref[:, lanes] = (stream_ref[:, lanes].astype(jnp.float32) + total).astype(jnp.bfloat16)


def natural(own, other, core, axis):
    return jnp.where(
        core == 0,
        jnp.concatenate([own, other], axis=axis),
        jnp.concatenate([other, own], axis=axis),
    )


def layer(
    resid,
    recurrent_input,
    recurrent_out_gate,
    filter_weight,
    recurrence_gate_matrix,
    input_gate_matrix,
    channel_decay_raw,
    token_decay_boost,
    output_projection_weight,
    expert_norm_gain,
    routes,
    expert_pair_weight,
    gate_weight,
    up_weight,
    down_weight,
):
    tokens, channels = recurrent_input.shape
    tp, experts = lax.axis_size("tp"), lax.axis_size("sp")
    here, place = lax.axis_index("tp"), lax.axis_index("sp")
    core = here % CORES
    chips = tp // CORES
    groups = core_groups(tp)
    rows_dev, width = resid.shape
    f32, bf16 = jnp.float32, jnp.bfloat16

    before = shifted(recurrent_input[tokens - RIM :], "sp", 1)
    quads = [[k * QUAD + i for i in range(QUAD)] for k in range(tp // QUAD)]
    strides = [[k * QUAD + i for k in range(tp // QUAD)] for i in range(QUAD)]
    projection = lax.all_gather(
        output_projection_weight, "tp", axis=0, axis_index_groups=quads, tiled=True
    )

    whole = lambda *shape: pl.BlockSpec(shape, lambda k: (0,) * len(shape))
    operands = (
        recurrent_input,
        before,
        filter_weight,
        recurrence_gate_matrix,
        input_gate_matrix,
        channel_decay_raw[None, :],
        token_decay_boost,
    )
    shapes = ((tokens, channels), (tokens, channels), (experts, 2, channels))
    state, running, total = pl.pallas_call(
        recurrence_kernel,
        out_shape=tuple(jax.ShapeDtypeStruct(shape, f32) for shape in shapes),
        in_specs=[VMEM] * len(operands),
        out_specs=(VMEM,) * len(shapes),
        scratch_shapes=[
            pltpu.VMEM((tokens + 8, channels), f32),
            pltpu.VMEM((tokens, channels), f32),
            pltpu.VMEM((tokens, channels), f32),
            pltpu.VMEM((channels, 2 * channels), bf16),
        ],
        cost_estimate=pl.CostEstimate(flops=10**9, bytes_accessed=2**20, transcendentals=0),
        name="recurrence",
    )(*operands)

    pieces = lax.all_to_all(total, "sp", 0, 0, tiled=True)
    held = lax.optimization_barrier((gate_weight[0], up_weight[0], total))
    gate_other, up_other = swap_cores(held[0]), swap_cores(held[1])
    own_routes = lax.dynamic_slice_in_dim(routes, here * rows_dev, rows_dev, 0)
    own_routes, pair = lax.optimization_barrier((own_routes, expert_pair_weight, total))[:2]
    column, line, pair = pl.pallas_call(
        slots_kernel,
        out_shape=(
            jax.ShapeDtypeStruct((2 * rows_dev, 1), jnp.int32),
            jax.ShapeDtypeStruct((2, PIECES * rows_dev), jnp.int32),
            jax.ShapeDtypeStruct(pair.shape, f32),
        ),
        in_specs=[VMEM] * 2,
        out_specs=(VMEM,) * 3,
        name="slots",
    )(own_routes, pair)
    branch = pl.pallas_call(
        branch_kernel,
        out_shape=jax.ShapeDtypeStruct((QUAD, tokens // QUAD, channels), bf16),
        in_specs=[SMEM] + [VMEM] * 4,
        out_specs=VMEM,
        name="branch",
    )(place.astype(jnp.int32)[None], pieces, state, running, recurrent_out_gate)
    mine = lax.all_to_all(branch, "tp", 0, 0, axis_index_groups=quads, tiled=True)
    cut = width // 2
    partial = pl.pallas_call(
        project_kernel,
        grid=(width // cut,),
        out_shape=jax.ShapeDtypeStruct((tokens // QUAD, width), bf16),
        in_specs=[
            pl.BlockSpec(mine.shape, lambda k: (0, 0, 0)),
            pl.BlockSpec((QUAD * channels, cut), lambda k: (0, k)),
        ],
        out_specs=pl.BlockSpec((tokens // QUAD, cut), lambda k: (0, k)),
        name="project",
    )(mine, projection)
    parts = lax.all_to_all(
        partial.reshape(tp // QUAD, rows_dev, width), "tp", 0, 0,
        axis_index_groups=strides, tiled=True,
    )
    slot_count = experts * CAP
    stream, outgoing = pl.pallas_call(
        dispatch_kernel,
        out_shape=(
            jax.ShapeDtypeStruct((rows_dev, width), bf16),
            jax.ShapeDtypeStruct((slot_count * PIECES, width // PIECES), bf16),
        ),
        in_specs=[VMEM] * 4,
        out_specs=(VMEM,) * 2,
        name="dispatch",
    )(parts, resid, expert_norm_gain[None, :], line)
    packed = (experts, CAP * PIECES, width // PIECES)
    arrived = lax.all_to_all(outgoing.reshape(packed), "sp", 0, 0, tiled=True)
    arrived = arrived.reshape(slot_count, width)

    rows = lax.all_gather(arrived, "tp", axis=0, axis_index_groups=groups, tiled=True)
    arrived, down_part, gate_own, up_own, gate_other, up_other = lax.optimization_barrier(
        (arrived, down_weight[0], gate_weight[0], up_weight[0], gate_other, up_other)
    )
    hidden = gate_own.shape[1]
    down_own = lax.all_to_all(
        down_part.reshape(chips, CORES * hidden, -1), "tp", 0, 0,
        axis_index_groups=groups, tiled=True,
    )
    gate = natural(gate_own, gate_other, core, 1)
    upward = natural(up_own, up_other, core, 1)
    down = natural(down_own[:, None], swap_cores(down_own)[:, None], core, 1)
    down = jnp.moveaxis(down.reshape(tp, CORES * hidden, -1), 0, 1).reshape(CORES * hidden, width)
    depth = CORES * hidden
    block = rows.shape[0] // EXPERT_STEPS
    summed = pl.pallas_call(
        expert_kernel,
        grid=(EXPERT_STEPS,),
        out_shape=jax.ShapeDtypeStruct(rows.shape, bf16),
        in_specs=[
            pl.BlockSpec((block, width), lambda k: (k, 0)),
            whole(width, depth),
            whole(width, depth),
            whole(depth, width),
        ],
        out_specs=pl.BlockSpec((block, width), lambda k: (k, 0)),
        name="experts",
    )(rows, gate, upward, down)
    result = lax.psum_scatter(
        summed, "tp", scatter_dimension=0, axis_index_groups=groups, tiled=True
    )

    returned = lax.all_to_all(result.reshape(packed), "sp", 0, 0, tiled=True)
    return pl.pallas_call(
        combine_kernel,
        out_shape=jax.ShapeDtypeStruct((rows_dev, width), bf16),
        in_specs=[VMEM] * 4,
        out_specs=VMEM,
        name="combine",
    )(stream, returned.reshape(slot_count * PIECES, width // PIECES), column, pair)


def solution(mesh):
    placed = (
        P(("sp", "tp"), None),
        P("sp", "tp"),
        P("sp", "tp"),
        P(None, "tp"),
        P("tp", None, None),
        P("tp", None, None),
        P("tp"),
        P("sp", "tp"),
        P("tp", None),
        P(),
        P("sp", None),
        P(("sp", "tp"), None),
        P("sp", None, "tp"),
        P("sp", None, "tp"),
        P("sp", None, "tp"),
    )
    return jax.shard_map(
        layer, mesh=mesh, in_specs=placed, out_specs=P(("sp", "tp"), None), check_vma=False
    )
```
